32 devices in a mesh: grp: 2 (over y), fs: 4 (over z), tp: 4 (over x, core).
Axes of the slice: x: 2, y: 2, z: 4, core: 2. Of those that a mesh axis runs over, the one named last changes fastest.
Arguments:
- tokens: bfloat16 [1024, 2048], P(('grp', 'fs')), parts along dimension 0, may hold values from -12 to 12, as said below
- mix_heads: bfloat16 [1024, 2048], P(('grp', 'fs'), 'tp'), parts along dimension 0, may hold values from -6 to 6
- norm_first: float32 [2048], replicated, may hold values from 0.1 to 1.9
- gate_first: bfloat16 [2048, 5632], P('fs', 'tp'), may hold values from -0.125 to 0.125
- up_first: bfloat16 [2048, 5632], P('fs', 'tp'), may hold values from -0.125 to 0.125
- down_first: bfloat16 [5632, 2048], P('tp', 'fs'), may hold values from -0.078125 to 0.078125
- out_weight: bfloat16 [2048, 2048], P('tp', 'fs'), may hold values from -0.125 to 0.125
- norm_second: float32 [2048], replicated, may hold values from 0.1 to 1.9
- gate_second: bfloat16 [2048, 5632], P('fs', 'tp'), may hold values from -0.125 to 0.125
- up_second: bfloat16 [2048, 5632], P('fs', 'tp'), may hold values from -0.125 to 0.125
- down_second: bfloat16 [5632, 2048], P('tp', 'fs'), may hold values from -0.078125 to 0.078125
Outputs:
- layer_out: bfloat16 [1024, 2048], P(('grp', 'fs')), parts along dimension 0
The draws below stay inside these ranges and needn't reach their ends.
There are 2 independent parts, one for each index of `grp`. The reference program is written for one: setup_inputs(seed, part) draws one part's arguments, and reference() takes and returns one part's arrays. A program takes and returns all parts, laid end to end along the dimension named above; an argument that names none is the same for every part. Nothing has to cross between parts.
Inputs may be any that keep to these rules, and one draw needn't show every extreme that they name: Each row of tokens carries a scale of its own.
All inputs are finite; a program needn't handle non-finite values.
Results may differ from the reference program's by a relative error of at most 0.014.
Values may be sent and summed in bfloat16 or wider, within the bound.
A program may use at most 64 MiB of HBM per device.

```python
import math
import jax
import jax.numpy as jnp
from jax import lax

D = 2048
FF = 5632
MIX = 2048
TOKENS = 512
N_TP = 4


def draw_tokens(key, part):
    subkeys = jax.random.split(key, 3)
    base_values = jax.random.normal(subkeys[0], (TOKENS, D), jnp.float32)
    row_scale = jnp.exp(jax.random.uniform(subkeys[1], (TOKENS, 1), jnp.float32, math.log(0.4), math.log(2.5)))
    values = base_values * row_scale
    return jnp.clip(values, -12.0, 12.0).astype(jnp.bfloat16)


def levels(key, dims, cuts, smallest, largest):
    loudness, own = 1.0, jax.random.fold_in(key, 6)
    for position, shards_of in cuts:
        steps = jnp.exp(jax.random.uniform(jax.random.fold_in(own, position), (shards_of,), jnp.float32, smallest / len(cuts), largest / len(cuts)))
        loudness = loudness * jnp.repeat(steps, dims[position] // shards_of).reshape([-1 if axis == position else 1 for axis in range(len(dims))])
    return loudness


def centred(stream_key, dims, deviation, most, cuts=(), dtype=jnp.bfloat16):
    level = levels(stream_key, dims, cuts, -0.22, 0.18) if cuts else 1.0
    entries = jax.random.normal(stream_key, dims, jnp.float32) * deviation * level
    return jnp.minimum(jnp.maximum(entries, -most), most).astype(dtype)


def setup_inputs(seed: int = 0, part: int = 0) -> dict:
    keys = jax.random.split(jax.random.key(seed), 12)
    part_keys = jax.random.split(jax.random.fold_in(keys[11], part), 12)
    return {
        "tokens": draw_tokens(jax.random.fold_in(jax.random.fold_in(keys[11], part), 71), part),
        "mix_heads": centred(part_keys[1], (TOKENS, MIX), 1.0, 6.0, ((0, 4), (1, 4))),
        "norm_first": jnp.clip(1.0 + 0.18 * jax.random.normal(keys[2], (D,), jnp.float32), 0.1, 1.9),
        "gate_first": centred(keys[3], (D, FF), D ** -0.5, 0.125, ((0, 4), (1, 4))),
        "up_first": centred(keys[4], (D, FF), D ** -0.5, 0.125, ((0, 4), (1, 4))),
        "down_first": centred(keys[5], (FF, D), FF ** -0.5, 0.078125, ((0, 4), (1, 4))),
        "out_weight": centred(keys[6], (MIX, D), MIX ** -0.5, 0.125, ((0, 4), (1, 4))),
        "norm_second": jnp.clip(1.0 + 0.18 * jax.random.normal(keys[7], (D,), jnp.float32), 0.1, 1.9),
        "gate_second": centred(keys[8], (D, FF), D ** -0.5, 0.125, ((0, 4), (1, 4))),
        "up_second": centred(keys[9], (D, FF), D ** -0.5, 0.125, ((0, 4), (1, 4))),
        "down_second": centred(keys[10], (FF, D), FF ** -0.5, 0.078125, ((0, 4), (1, 4))),
    }


EPS = 0.1

def norm_rows(row_block, gain_vector):
    widened = row_block.astype(jnp.float32)
    scaled = widened * lax.rsqrt(lax.optimization_barrier(jnp.mean(widened * widened, axis=-1, keepdims=True)) + EPS)
    return (scaled * gain_vector.astype(jnp.float32)).astype(jnp.bfloat16)

def branch_terms(normed, gate_weight, value_weight, down_weight, added_term):
    block_width = FF // N_TP

    def block_term(index):
        first_col = (index * block_width).astype(jnp.int32)
        gates = jnp.dot(normed, lax.dynamic_slice_in_dim(gate_weight, first_col, block_width, 1), preferred_element_type=jnp.float32)
        values = jnp.dot(normed, lax.dynamic_slice_in_dim(value_weight, first_col, block_width, 1), preferred_element_type=jnp.float32)
        hidden = (jax.nn.silu(gates) * values).astype(jnp.bfloat16)
        partial_value = 0.5 * jnp.dot(hidden, lax.dynamic_slice_in_dim(down_weight, first_col, block_width, 0), preferred_element_type=jnp.float32)
        return partial_value + added_term(index)

    def accumulate(index, total):
        rounded = lax.optimization_barrier(block_term(index).astype(jnp.bfloat16))
        return total + rounded.astype(jnp.float32)
    start_total = jnp.zeros((normed.shape[0], down_weight.shape[1]), jnp.float32)
    return lax.fori_loop(0, N_TP, accumulate, start_total)

def reference(tokens, mix_heads, norm_first, gate_first, up_first, down_first, out_weight, norm_second, gate_second, up_second, down_second):
    head_width = MIX // N_TP

    def head_term(index):
        first_col = (index * head_width).astype(jnp.int32)
        heads = lax.dynamic_slice_in_dim(mix_heads, first_col, head_width, 1)
        weight_rows = lax.dynamic_slice_in_dim(out_weight, first_col, head_width, 0)
        return jnp.dot(heads, weight_rows, preferred_element_type=jnp.float32)

    def no_term(index):
        return jnp.zeros((tokens.shape[0], tokens.shape[1]), jnp.float32)
    normed_one = norm_rows(tokens, norm_first)
    mixed_sum = branch_terms(normed_one, gate_first, up_first, down_first, head_term)
    resid_two = tokens.astype(jnp.float32) + mixed_sum
    normed_two = norm_rows(resid_two, norm_second)
    ffn_sum = branch_terms(normed_two, gate_second, up_second, down_second, no_term)
    return (resid_two + ffn_sum).astype(jnp.bfloat16)
```

```python
import functools

import jax
import jax.numpy as jnp
from jax import lax
from jax.experimental import pallas as pl
from jax.experimental.pallas import tpu as pltpu
from jax.sharding import PartitionSpec as P

EPS = 0.1
MESH = pl.DeviceIdType.MESH
BF16 = jnp.bfloat16
F32 = jnp.float32


def loop(count, body):
    def step(i, carry):
        body(i)
        return carry

    lax.fori_loop(0, count, step, 0)


def kernel(n_fs, n_tp, chunk,
           tok, mix, gain1, wg1, wu1, wd1, wo, gain2, wg2, wu2, wd2,
           out,
           vg1, vu1, vd1, vo, vg2, vu2, vd2,
           raw, nb2, mixed, grads, sums, in1, in2, hid1, hid2,
           terms, got1, got2, resid, squares1, squares, done_rows, joined,
           wsem, p0_send, p0_recv, fw_send, fw_recv, s1_send, s1_recv, mix_send, mix_recv,
           rs_send, rs_recv, ag_send, ag_recv, tp_send, tp_recv,
           sq_send, sq_recv, nrm_send, nrm_recv, nfw_send, nfw_recv,
           out_send, out_recv, ofw_send, ofw_recv):
    f, t = lax.axis_index("fs"), lax.axis_index("tp")
    rows_in, width = tok.shape
    total = rows_in * n_fs
    share = total // n_tp
    half = total // 2
    n_chunks = half // chunk
    dc = width // n_fs

    weights = ((wg1, vg1), (wu1, vu1), (wd1, vd1), (wo, vo), (wg2, vg2), (wu2, vu2), (wd2, vd2))
    loads = [pltpu.make_async_copy(a, b, wsem.at[i]) for i, (a, b) in enumerate(weights)]
    for load in loads:
        load.start()

    barrier = pltpu.get_barrier_semaphore()

    def greet(i):
        pf, pt = i // n_tp, i % n_tp

        @pl.when(jnp.logical_or(pf != f, pt != t))
        def _():
            pl.semaphore_signal(barrier, inc=1, device_id={"fs": pf, "tp": pt}, device_id_type=MESH)

    loop(n_fs * n_tp, greet)

    def cols(j):
        return pl.ds(pl.multiple_of(j * dc, dc), dc)

    def block(j, size):
        return pl.ds(pl.multiple_of(j * size, size), size)

    def remote(src, dst, send, recv, **where):
        return pltpu.make_async_remote_copy(
            src_ref=src, dst_ref=dst, send_sem=send, recv_sem=recv,
            device_id=where, device_id_type=MESH)

    c_own = t % 2
    partner = t + 1 - 2 * c_own
    half_in = rows_in // 2
    n_pairs = n_tp // 2

    def squares_of(x):
        own = jnp.sum(x * x, axis=-1, keepdims=True)
        return jnp.transpose(jnp.broadcast_to(own, (x.shape[0], 128)))[0:8, :]

    def scale_of(summed):
        column = jnp.transpose(jnp.broadcast_to(summed[0:1, :], (128, summed.shape[1])))[:, 0:1]
        return lax.rsqrt(column * (1.0 / width) + EPS)

    def piece_of(slot):
        return pl.ds(pl.multiple_of(slot * rows_in + c_own * half_in, half_in), half_in)

    def p0_copy(j, slot):
        return remote(tok.at[block(c_own, half_in), cols(j)], raw.at[piece_of(slot), :],
                      p0_send.at[j], p0_recv.at[slot], fs=j)

    def fw_copy(slot):
        place = raw.at[piece_of(slot), :]
        return remote(place, place, fw_send.at[slot], fw_recv.at[slot], tp=partner)

    def s1_copy(j, slot):
        return remote(squares1.at[f], squares1.at[slot], s1_send.at[j], s1_recv.at[slot], fs=j)

    def sq_copy(j, slot):
        return remote(squares.at[f], squares.at[slot], sq_send.at[j], sq_recv.at[slot], fs=j)

    def mix_copy(slot, side, where):
        place = mixed.at[block(slot, rows_in), :]
        return remote(place, place, mix_send.at[slot, side], mix_recv.at[slot], fs=where)

    mixed[block(f, rows_in), :] = mix[...]
    pl.semaphore_wait(barrier, n_fs * n_tp - 1)

    def p0_start(i):
        p0_copy((f + 1 + i) % n_fs, f).start()

    loop(n_fs - 1, p0_start)
    squares1[f] = squares_of(tok[...].astype(F32))

    def s1_start(i):
        s1_copy((f + 1 + i) % n_fs, f).start()

    loop(n_fs - 1, s1_start)

    @pl.when(f < n_fs - 1)
    def _():
        mix_copy(f, 0, f + 1).start()

    @pl.when(f > 0)
    def _():
        mix_copy(f, 1, f - 1).start()

    raw[block(f, rows_in), :] = tok[:, cols(f)]

    def gates_one(j):
        rows = block(j, rows_in)
        x = (raw[rows, :].astype(F32) * scale_of(squares1[j]) * gain1[:, cols(f)]).astype(BF16)
        grads[0, rows, :] = jnp.dot(x, vg1[...], preferred_element_type=F32)
        grads[1, rows, :] = jnp.dot(x, vu1[...], preferred_element_type=F32)

    def side_of(side):
        hops = jnp.where(side == 0, n_fs - 1 - f, f)
        toward = jnp.where(side == 0, f - 1, f + 1)
        away = jnp.where(side == 0, f + 1, f - 1)
        return hops, toward, away

    near = jnp.where(2 * f >= n_fs, 0, 1)

    def chain(layer, arrived, hid, with_mix):
        def rows_of(side, c):
            return pl.ds(pl.multiple_of(side * half + c * chunk, chunk), chunk)

        def rs_copy(side, c, where):
            rows = rows_of(side, c)
            return remote(sums.at[:, rows, :], arrived.at[:, rows, :],
                          rs_send.at[layer, side, c], rs_recv.at[layer, side, c], fs=where)

        def ag_copy(side, c, where):
            rows = rows_of(side, c)
            return remote(hid.at[rows, :], hid.at[rows, :],
                          ag_send.at[layer, side, c], ag_recv.at[layer, side, c], fs=where)

        for side in (0, 1):
            hops, toward, away = side_of(side)

            @pl.when(hops == 0)
            def _():
                def first(c):
                    rows = rows_of(side, c)
                    sums[:, rows, :] = grads[:, rows, :].astype(BF16)
                    rs_copy(side, c, toward).start()

                loop(n_chunks, first)

        def step(s):
            for k in (0, 1):
                side = near if k == 0 else 1 - near
                hops, toward, away = side_of(side)
                c = s - hops

                @pl.when(jnp.logical_and(hops > 0, jnp.logical_and(c >= 0, c < n_chunks)))
                def _():
                    rows = rows_of(side, c)
                    rs_copy(side, c, f).wait_recv()

                    @pl.when(hops < n_fs - 1)
                    def _():
                        sums[:, rows, :] = (grads[:, rows, :] + arrived[:, rows, :].astype(F32)).astype(BF16)
                        rs_copy(side, c, toward).start()

                    @pl.when(hops == n_fs - 1)
                    def _():
                        g = grads[0, rows, :] + arrived[0, rows, :].astype(F32)
                        v = grads[1, rows, :] + arrived[1, rows, :].astype(F32)
                        hid[rows, :] = (g / (1.0 + jnp.exp(-g)) * v).astype(BF16)
                        ag_copy(side, c, away).start()

            if with_mix:
                @pl.when(jnp.logical_and(s > 0, s < n_fs))
                def _():
                    low, high = f - s, f + s

                    @pl.when(low >= 0)
                    def _():
                        mix_copy(low, 0, f).wait_recv()

                        @pl.when(f < n_fs - 1)
                        def _():
                            mix_copy(low, 0, f + 1).start()

                    @pl.when(high < n_fs)
                    def _():
                        mix_copy(high, 1, f).wait_recv()

                        @pl.when(f > 0)
                        def _():
                            mix_copy(high, 1, f - 1).start()

        loop(n_chunks + n_fs - 1, step)

        def relay(c):
            for k in (0, 1):
                side = 1 - near if k == 0 else near
                hops, toward, away = side_of(side)

                @pl.when(hops < n_fs - 1)
                def _():
                    ag_copy(side, c, f).wait_recv()

                    @pl.when(hops > 0)
                    def _():
                        ag_copy(side, c, away).start()

        def drain(c):
            for side in (0, 1):
                hops, toward, away = side_of(side)

                @pl.when(hops < n_fs - 1)
                def _():
                    rs_copy(side, c, f).wait_send()

                @pl.when(hops > 0)
                def _():
                    ag_copy(side, c, f).wait_send()

        return relay, lambda: loop(n_chunks, drain)

    def tp_copy(layer, j, slot, got):
        return remote(terms.at[block(j, share), :], got.at[slot],
                      tp_send.at[layer, j], tp_recv.at[layer, slot], tp=j)

    def down(layer, relay, hid, vd, got, with_mix):
        per_block = n_chunks // n_pairs

        def piece(b):
            def inner(i):
                relay(b * per_block + i)

            loop(per_block, inner)
            for side in (0, 1):
                j = side * n_pairs + b
                rows = block(j, share)
                value = 0.5 * jnp.dot(hid[rows, :], vd[...], preferred_element_type=F32)
                if with_mix:
                    value = value + jnp.dot(mixed[rows, :], vo[...], preferred_element_type=F32)
                terms[rows, :] = value.astype(BF16)

                @pl.when(j != t)
                def _():
                    tp_copy(layer, j, t, got).start()

        loop(n_pairs, piece)

    def reduce_tp(layer, got, start_value):
        resid[...] = start_value + terms[block(t, share), :].astype(F32)

        def add(i):
            j = (t + 1 + i) % n_tp
            tp_copy(layer, j, j, got).wait_recv()
            resid[...] = resid[...] + got[j].astype(F32)

        loop(n_tp - 1, add)

        def drain(i):
            j = (t + 1 + i) % n_tp
            tp_copy(layer, j, t, got).wait_send()

        loop(n_tp - 1, drain)

    loads[0].wait()
    loads[1].wait()
    gates_one(f)

    def pass_on(i):
        j = (f + 1 + i) % n_fs
        p0_copy(j, j).wait_recv()
        fw_copy(j).start()

    loop(n_fs - 1, pass_on)

    def other_rows(i):
        j = (f + 1 + i) % n_fs
        s1_copy(j, j).wait_recv()
        fw_in(j).wait_recv()
        gates_one(j)

    def fw_in(slot):
        start = pl.multiple_of(slot * rows_in + (1 - c_own) * half_in, half_in)
        place = raw.at[pl.ds(start, half_in), :]
        return remote(place, place, fw_send.at[slot], fw_recv.at[slot], tp=partner)

    loop(n_fs - 1, other_rows)
    relay_one, drain_one = chain(0, in1, hid1, True)
    loads[2].wait()
    loads[3].wait()
    down(0, relay_one, hid1, vd1, got1, True)
    reduce_tp(0, got1, raw[block(t, share), :].astype(F32))

    squares[f] = squares_of(resid[...])

    def sq_start(i):
        sq_copy((f + 1 + i) % n_fs, f).start()

    def sq_wait(i):
        j = (f + 1 + i) % n_fs
        sq_copy(j, j).wait_recv()

    loop(n_fs - 1, sq_start)
    drain_one()
    loop(n_fs - 1, sq_wait)
    summed = squares[0]
    for j in range(1, n_fs):
        summed = summed + squares[j]
    nb2[block(t, share), :] = (resid[...] * scale_of(summed) * gain2[:, cols(f)]).astype(BF16)

    def nrm_copy(j, slot):
        place = nb2.at[block(slot, share), :]
        return remote(place, place, nrm_send.at[j], nrm_recv.at[slot], tp=j)

    def nfw_copy(slot):
        place = nb2.at[block(slot, share), :]
        return remote(place, place, nfw_send.at[slot], nfw_recv.at[slot], tp=partner)

    def same_core(i):
        return (t + 2 + 2 * i) % n_tp

    def nrm_start(i):
        nrm_copy(same_core(i), t).start()

    loop(n_pairs - 1, nrm_start)
    nfw_copy(t).start()
    loads[4].wait()
    loads[5].wait()

    def gates_two(j):
        rows = block(j, share)
        x = nb2[rows, :]
        grads[0, rows, :] = jnp.dot(x, vg2[...], preferred_element_type=F32)
        grads[1, rows, :] = jnp.dot(x, vu2[...], preferred_element_type=F32)

    gates_two(t)
    nfw_copy(partner).wait_recv()
    gates_two(partner)

    def nrm_pass(i):
        j = same_core(i)
        nrm_copy(j, j).wait_recv()
        nfw_copy(j).start()
        gates_two(j)

    loop(n_pairs - 1, nrm_pass)

    def nrm_last(i):
        j = (partner + 2 + 2 * i) % n_tp
        nfw_copy(j).wait_recv()
        gates_two(j)

    loop(n_pairs - 1, nrm_last)
    relay_two, drain_two = chain(1, in2, hid2, False)
    loads[6].wait()
    down(1, relay_two, hid2, vd2, got2, False)
    reduce_tp(1, got2, resid[...])
    done_rows[...] = resid[...].astype(BF16)

    def out_copy(j, slot):
        return remote(done_rows, joined.at[:, cols(slot)], out_send.at[j], out_recv.at[slot], fs=t, tp=j)

    def ofw_copy(slot):
        place = joined.at[:, cols(slot)]
        return remote(place, place, ofw_send.at[slot], ofw_recv.at[slot], tp=partner)

    def out_start(i):
        j = c_own + 2 * i

        @pl.when(jnp.logical_or(f != t, j != t))
        def _():
            out_copy(j, f).start()

    loop(n_pairs, out_start)

    @pl.when(f == t)
    def _():
        joined[:, cols(f)] = done_rows[...]

    takes = c_own == f % 2

    @pl.when(takes)
    def _():
        def take(i):
            j = (f + i) % n_fs

            @pl.when(jnp.logical_or(f != t, j != f))
            def _():
                out_copy(t, j).wait_recv()

            ofw_copy(j).start()

        loop(n_fs, take)

    @pl.when(jnp.logical_not(takes))
    def _():
        def take(i):
            ofw_copy((f + i) % n_fs).wait_recv()

        loop(n_fs, take)

    out[...] = joined[...]

    drain_two()

    def last_fs(i):
        j = (f + 1 + i) % n_fs
        p0_copy(j, f).wait_send()
        fw_copy(j).wait_send()
        s1_copy(j, f).wait_send()
        sq_copy(j, f).wait_send()

    loop(n_fs - 1, last_fs)

    def last_mix(j):
        @pl.when(jnp.logical_and(j <= f, f < n_fs - 1))
        def _():
            mix_copy(j, 0, f).wait_send()

        @pl.when(jnp.logical_and(j >= f, f > 0))
        def _():
            mix_copy(j, 1, f).wait_send()

        @pl.when(takes)
        def _():
            ofw_copy(j).wait_send()

    loop(n_fs, last_mix)

    def last_nrm(i):
        nrm_copy(same_core(i), t).wait_send()

    loop(n_pairs - 1, last_nrm)

    def last_out(i):
        j = c_own + 2 * i
        nfw_copy(j).wait_send()

        @pl.when(jnp.logical_or(f != t, j != t))
        def _():
            out_copy(j, f).wait_send()

    loop(n_pairs, last_out)


def by_count(counts, value, body):
    for n in counts:
        if len(counts) == 1:
            body(n)
        else:
            pl.when(value == n)(functools.partial(body, n))


def gathered(counts, n_fs, n_tp, n_q, lane,
             tok, mix, gain1, wg1, wu1, wd1, wo, gain2, wg2, wu2, wd2,
             out,
             rows_of_me, wgu, wdb, wob, xs, mixed, hid, acc, part, r1, s1, r2, full, zs, rp, rr, zf, rf, resid, done, joined,
             tok_sem, mix_sem, write_sem, wl_sem, dl_sem, wo_sem,
             wz_send, wz_recv, wy_send, wy_recv, dz_send, dz_recv, dy_send, dy_recv,
             ag_send, ag_recv, agr_send, ax_send, ax_recv, ad_send, ad_recv, af_send, af_recv,
             mz_send, mz_recv, mr_send,
             r1_send, r1_recv, r2_send, r2_recv, rp_send, rp_recv, rr_send, rr_recv, rf_send, rf_recv,
             o_send, o_recv):
    g, f, t = lax.axis_index("grp"), lax.axis_index("fs"), lax.axis_index("tp")
    rows_in, width = tok.shape
    dc, hidden = wg1.shape
    n_x = n_tp // 2
    core, x = t % 2, t // 2
    sub = rows_in // n_tp
    unit = n_fs * sub
    u = core * n_x + x
    u_x = core * n_x + 1 - x
    u_pair = (1 - core) * n_x + x
    u_diag = (1 - core) * n_x + 1 - x
    t_x = (t + 2) % n_tp
    t_pair = t + 1 - 2 * core
    t_diag = (t_pair + 2) % n_tp
    pair = f + 1 - 2 * (f % 2)
    far0 = jnp.where(f < 2, 2, 0)
    inner = jnp.logical_or(f == 1, f == 2)
    bridge = jnp.where(f < 2, 2, 1)
    others = (n_fs - 1 - f, (f + 2) % n_fs, pair)
    n_k = 4
    piece = dc // (2 * n_k)
    qc = dc // n_q
    n_lane = hidden // lane
    most = max(counts)
    gate_up = ((wg1, wu1), (wg2, wu2))
    downs = (wd1, wd2)

    def first(j):
        return (j * n_lane + (1 - core) * (n_fs - 1)) // n_fs

    def count(j):
        return first(j + 1) - first(j)

    mine = count(f)

    def at(i, size):
        return pl.ds(pl.multiple_of(i * size, size), size)

    def remote(src, dst, send, recv, **where):
        return pltpu.make_async_remote_copy(
            src_ref=src, dst_ref=dst, send_sem=send, recv_sem=recv,
            device_id=where, device_id_type=MESH)

    def load_gate_up(n, l, m):
        cols = pl.ds(pl.multiple_of(first(f) * lane, lane), n * lane)
        return pltpu.make_async_copy(
            gate_up[l][m].at[:, cols], wgu.at[l, m, at(f, dc), pl.ds(0, n * lane)], wl_sem.at[l, m])

    def load_down(n, l, q):
        rows = pl.ds(pl.multiple_of(first(f) * lane, lane), n * lane)
        return pltpu.make_async_copy(
            downs[l].at[rows, at(q, qc)], wdb.at[l, q, pl.ds(0, n * lane), at(f, qc)], dl_sem.at[l, q])

    def start_loads(n):
        for l in (0, 1):
            for m in (0, 1):
                load_gate_up(n, l, m).start()
            for q in range(n_q):
                load_down(n, l, q).start()
        if n < most:
            rest = pl.ds(n * lane, (most - n) * lane)
            wgu[:, :, :, rest] = jnp.zeros((2, 2, width, (most - n) * lane), BF16)
            wdb[:, :, rest, :] = jnp.zeros((2, n_q, (most - n) * lane, n_fs * qc), BF16)

    barrier = pltpu.get_barrier_semaphore()
    for i in range(n_fs - 1):
        pl.semaphore_signal(barrier, inc=1, device_id={"fs": others[i]}, device_id_type=MESH)
    pl.semaphore_signal(barrier, inc=1, device_id={"grp": 1 - g}, device_id_type=MESH)
    for j in (t_x, t_pair, t_diag):
        pl.semaphore_signal(barrier, inc=1, device_id={"tp": j}, device_id_type=MESH)

    load_tok = pltpu.make_async_copy(tok, rows_of_me, tok_sem)
    load_tok.start()
    load_mix = [pltpu.make_async_copy(
        mix.at[j * sub:(j + 1) * sub, :], mixed.at[(j % 2) * n_x + j // 2, f], mix_sem) for j in range(n_tp)]
    for load in load_mix:
        load.start()
    by_count(counts, mine, start_loads)
    load_out = pltpu.make_async_copy(wo, wob, wo_sem)
    load_out.start()

    def normed(values, gain):
        squares = jnp.sum(values * values, axis=-1, keepdims=True)
        return values * lax.rsqrt(squares * (1.0 / width) + EPS) * gain

    load_tok.wait()
    own = rows_of_me[at(t, sub), :].astype(F32)
    xs[0, u, f] = normed(own, gain1[...]).astype(BF16)
    for j in range(n_tp):
        @pl.when(j != t)
        def _():
            rows = rows_of_me[j * sub:(j + 1) * sub, :].astype(F32)
            xs[0, (j % 2) * n_x + j // 2, f] = normed(rows, gain1[...]).astype(BF16)
    for q in range(n_q):
        for j in range(n_fs):
            resid[q, :, j * qc:(j + 1) * qc] = own[:, j * dc + q * qc:j * dc + (q + 1) * qc]
    pltpu.make_async_copy(mixed.at[:, f], mixed.at[:, f], mix_sem).wait()
    pl.semaphore_wait(barrier, n_fs - 1 + 1 + n_tp - 1)

    def send_one(n, l, m, k, j):
        cols = pl.ds(pl.multiple_of(first(j) * lane, lane), n * lane)
        remote(gate_up[l][m].at[at(n_k * g + k, piece), cols],
               wgu.at[l, m, at(n_k * (2 * f + g) + k, piece), pl.ds(0, n * lane)],
               wz_send.at[l, j], wz_recv.at[l, m, k], fs=j).start()

    def send_gate_up(l, r, where=others):
        for j in where:
            by_count(counts, count(j), lambda n, j=j: send_one(n, l, r % 2, r // 2, j))

    def gate_up_y(n, l, m, k, j):
        place = wgu.at[l, m, at(n_k * (2 * j + g) + k, piece), pl.ds(0, n * lane)]
        return remote(place, place, wy_send.at[l], wy_recv.at[l, m, k], grp=1 - g)

    def all_pieces(n, l, m, k, send, recv):
        place = wgu.at[l, m, pl.ds(0, len(others) * piece), pl.ds(0, n * lane)]
        return remote(place, place, send, recv, grp=1 - g)

    def pass_gate_up(l, r):
        m, k = r % 2, r // 2

        def go(n):
            all_pieces(n, l, m, k, wz_send.at[l, pair], wz_recv.at[l, m, k]).wait_recv()
            for j in others:
                gate_up_y(n, l, m, k, j).start()

        by_count(counts, mine, go)

    def take_gate_up(l, r):
        m, k = r % 2, r // 2
        by_count(counts, mine, lambda n: all_pieces(n, l, m, k, wy_send.at[l], wy_recv.at[l, m, k]).wait_recv())

    def down_part(n, l, q, j, side):
        size = n * lane // 2
        return wdb.at[l, q, at(side, size), at(j, qc)]

    def send_down(l, q, where=others):
        for j in where:
            def go(n, j=j):
                size = n * lane // 2
                rows = pl.ds(pl.multiple_of(first(j) * lane + g * size, lane // 2), size)
                remote(downs[l].at[rows, at(q, qc)], down_part(n, l, q, f, g),
                       dz_send.at[l, j], dz_recv.at[l, q, f], fs=j).start()

            by_count(counts, count(j), go)

    def down_y(n, l, q, j):
        place = down_part(n, l, q, j, g)
        return remote(place, place, dy_send.at[l], dy_recv.at[l, q], grp=1 - g)

    def all_downs(n, l, q, send, recv):
        place = wdb.at[l, q, pl.ds(0, n * lane // 2), pl.ds(0, len(others) * qc)]
        return remote(place, place, send, recv, grp=1 - g)

    def z_block(l, j, h, send, where):
        place = xs.at[l, u, j, at(h, sub // 2)]
        return remote(place, place, send, ag_recv.at[l, j, h], fs=where)

    def x_block(l, j, who, h):
        place = xs.at[l, who, j, at(h, sub // 2)]
        return remote(place, place, ax_send.at[l], ax_recv.at[l, j, h], tp=t_x)

    def pair_block(l, j, who, h):
        place = xs.at[l, who, j, at(h, sub // 2)]
        return remote(place, place, ad_send.at[l], ad_recv.at[l], tp=t_pair)

    def diag_block(l, j, who, h):
        place = xs.at[l, who, j, at(h, sub // 2)]
        return remote(place, place, af_send.at[l], af_recv.at[l], tp=t_pair)

    def pass_rows(l, j, h):
        x_block(l, j, u, h).start()
        pair_block(l, j, u, h).start()

    def gather_own(l):
        for h in (0, 1):
            z_block(l, f, h, ag_send.at[l], bridge).start()
        for h in (0, 1):
            z_block(l, f, h, ag_send.at[l], pair).start()
            if l == 1:
                pass_rows(l, f, h)

    def gather_near(l):
        for h in (0, 1):
            for k in (0, 1):
                @pl.when(inner)
                def _():
                    j = far0 + k
                    z_block(l, j, h, agr_send.at[l], j).wait_recv()
                    z_block(l, j, h, agr_send.at[l], pair).start()
                    pass_rows(l, j, h)

        for h in (0, 1):
            z_block(l, pair, h, ag_send.at[l], pair).wait_recv()
            pass_rows(l, pair, h)

    def gather_far(l):
        for h in (0, 1):
            for k in (0, 1):
                @pl.when(jnp.logical_not(inner))
                def _():
                    j = far0 + k
                    z_block(l, j, h, agr_send.at[l], j).wait_recv()
                    pass_rows(l, j, h)

    def gather_end(l):
        blocks = [(j, h) for j in (far0, far0 + 1, pair) for h in (0, 1)]
        if l == 1:
            blocks = [(f, 0), (f, 1)] + blocks
        for j, h in blocks:
            x_block(l, j, u_x, h).wait_recv()
            diag_block(l, j, u_x, h).start()
        rows = xs.at[l, 0, pl.ds(0, len(blocks) // 2)]
        remote(rows, rows, ad_send.at[l], ad_recv.at[l], tp=t_pair).wait_recv()
        remote(rows, rows, af_send.at[l], af_recv.at[l], tp=t_pair).wait_recv()

    def mix_block(j, send, where):
        place = mixed.at[:, j]
        return remote(place, place, send, mz_recv.at[j], fs=where)

    def mix_near():
        @pl.when(inner)
        def _():
            for k in (0, 1):
                j = far0 + k
                mix_block(j, mr_send.at[k], j).wait_recv()
                mix_block(j, mr_send.at[k], pair).start()

    def mix_far():
        @pl.when(jnp.logical_not(inner))
        def _():
            for k in (0, 1):
                mix_block(far0 + k, mr_send.at[k], far0 + k).wait_recv()

        mix_block(pair, mz_send.at[1], pair).wait_recv()

    def hidden_of(l):
        def step(i):
            rows = xs[l, at(i, n_x)].reshape(n_x * unit, width)
            gate = jnp.dot(rows, wgu[l, 0], preferred_element_type=F32)
            value = jnp.dot(rows, wgu[l, 1], preferred_element_type=F32)
            hid[at(i, n_x * unit), :] = (gate / (1.0 + jnp.exp(-gate)) * value).astype(BF16)

        loop(2, step)

    def s1_copy(l, q):
        return remote(part.at[l, q, at(1 - core, n_x)], r1.at[l, q], r1_send.at[l], r1_recv.at[l, q], tp=t_pair)

    def s2_copy(l, q):
        return remote(s1.at[l, q], r2.at[l, q], r2_send.at[l], r2_recv.at[l, q], tp=t_x)

    def pair_copy(l, q):
        return remote(zs.at[l, q, pair], rp.at[l, q], rp_send.at[l], rp_recv.at[l, q], fs=pair)

    def relay_copy(l, q):
        return remote(zs.at[l, q, pl.ds(far0, 2)], rr.at[l, q], rr_send.at[l], rr_recv.at[l, q], fs=pair)

    def far_copy(l, q, k, where):
        return remote(zf.at[l, q, k], rf.at[l, q], rf_send.at[l], rf_recv.at[l, q], fs=where)

    def out_copy(q, where, who):
        return remote(done.at[q], joined.at[q, at(who, sub)], o_send, o_recv.at[q], tp=where)

    def pass_down(l, q):
        def go(n):
            for j in others:
                place = down_part(n, l, q, j, g)
                remote(place, place, dz_send.at[l, j], dz_recv.at[l, q, j], fs=j).wait_recv()
                down_y(n, l, q, j).start()

        by_count(counts, mine, go)

    def write_copy(q, j):
        return pltpu.make_async_copy(
            joined.at[q, :, at(j, qc)], out.at[:, pl.ds(pl.multiple_of(j * dc + q * qc, qc), qc)], write_sem)

    def reduced(l, hooks):
        def multiply(q):
            @pl.when(q < n_q - 1)
            def _():
                pass_down(l, q + 1)

            def ready(n):
                all_downs(n, l, q, dy_send.at[l], dy_recv.at[l, q]).wait_recv()
                load_down(n, l, q).wait()

            by_count(counts, mine, ready)

            def side(i):
                c = (1 - core) * (1 - i) + core * i
                value = 0.5 * jnp.dot(hid[at(c, n_x * unit), :], wdb[l, q], preferred_element_type=F32)
                if l == 0:
                    acc[...] = value
                    heads = mixed[at(c, n_x)].reshape(n_x * unit, mixed.shape[-1])
                    acc[:, at(f, qc)] = acc[:, at(f, qc)] + jnp.dot(
                        heads, wob[:, at(q, qc)], preferred_element_type=F32)
                    value = acc[...]
                part[l, q, at(c, n_x)] = value.astype(BF16).reshape(n_x, n_fs, sub, n_fs * qc)

                @pl.when(i == 0)
                def _():
                    s1_copy(l, q).start()

            loop(2, side)

        def across(q):
            s1_copy(l, q).wait_recv()
            s1[l, q] = (part[l, q, u_x].astype(F32) + r1[l, q, 1 - x].astype(F32)).astype(BF16)
            s2_copy(l, q).start()

        def along(q):
            s2_copy(l, q).wait_recv()
            value = part[l, q, u].astype(F32) + r1[l, q, x].astype(F32) + r2[l, q].astype(F32)
            full[l, q] = value
            zs[l, q] = value.astype(BF16)

            @pl.when(jnp.logical_not(inner))
            def _():
                relay_copy(l, q).start()

            pair_copy(l, q).start()

        def relay(q):
            @pl.when(inner)
            def _():
                relay_copy(l, q).wait_recv()
                for k in (0, 1):
                    zf[l, q, k] = (full[l, q, far0 + k] + rr[l, q, k].astype(F32)).astype(BF16)
                    far_copy(l, q, k, far0 + k).start()

        def finish(q):
            pair_copy(l, q).wait_recv()
            far_copy(l, q, 0, far0).wait_recv()
            value = full[l, q, f] + rp[l, q].astype(F32) + rf[l, q].astype(F32)
            value = resid[q] + value
            if l == 0:
                resid[q] = value
            else:
                done[q] = value.astype(BF16)
                joined[q, at(t, sub)] = value.astype(BF16)
                for where in (t_x, t_diag, t_pair):
                    out_copy(q, where, t).start()

        def write(q):
            rows = joined.at[q, pl.ds(0, (n_tp - 1) * sub)]
            remote(rows, rows, o_send, o_recv.at[q], tp=t_pair).wait_recv()
            for j in range(n_fs):
                write_copy(q, j).start()

        stages = [(multiply, 0), (across, 0), (along, 1), (relay, 2), (finish, 4 - l)]
        if l == 1:
            stages.append((write, 4))

        def step(s):
            for stage, lag in stages:
                @pl.when(jnp.logical_and(s >= lag, s < n_q + lag))
                def _():
                    stage(s - lag)

            for when, hook in hooks:
                pl.when(s == when)(hook)

        loop(n_q + stages[-1][1], step)

    def sent(ref, sem):
        remote(ref, ref, sem, ag_recv.at[0, 0, 0], tp=t_pair).wait_send()

    def drain_gate_up(l):
        for j in others:
            by_count(counts, count(j), lambda n, j=j: sent(
                wgu.at[l, 0, pl.ds(0, dc), pl.ds(0, n * lane)], wz_send.at[l, j]))
        by_count(counts, mine, lambda n: sent(
            wgu.at[l, 0, pl.ds(0, len(others) * dc), pl.ds(0, n * lane)], wy_send.at[l]))
        sent(xs.at[l, 0, pl.ds(0, 2)], ag_send.at[l])
        pl.when(inner)(lambda: sent(xs.at[l, 0, pl.ds(0, 2)], agr_send.at[l]))
        rows = xs.at[l, 0, pl.ds(0, 4 if l == 1 else 3)]
        for sem in (ax_send, ad_send, af_send):
            sent(rows, sem.at[l])

    def drain_mix():
        mix_block(f, mz_send.at[0], bridge).wait_send()
        mix_block(f, mz_send.at[1], pair).wait_send()

        @pl.when(inner)
        def _():
            for k in (0, 1):
                mix_block(far0 + k, mr_send.at[k], pair).wait_send()

    def drain_down(l):
        for j in others:
            by_count(counts, count(j), lambda n, j=j: sent(
                wdb.at[l, 0, pl.ds(0, n * lane // 2)], dz_send.at[l, j]))
        by_count(counts, mine, lambda n: sent(
            wdb.at[l, pl.ds(0, len(others)), pl.ds(0, n * lane // 2)], dy_send.at[l]))

    def drain_steps(l):
        sent(part.at[l, :, pl.ds(0, n_x)], r1_send.at[l])
        sent(s1.at[l], r2_send.at[l])
        sent(zs.at[l, 0], rp_send.at[l])
        pl.when(inner)(lambda: sent(zs.at[l, pl.ds(0, 2)], rf_send.at[l]))
        pl.when(jnp.logical_not(inner))(lambda: sent(zs.at[l, pl.ds(0, 2)], rr_send.at[l]))
        if l == 1:
            sent(joined.at[:, pl.ds(0, (n_tp - 1) * sub)], o_send)

    def wait_own(l):
        for m in (0, 1):
            by_count(counts, mine, lambda n, m=m: load_gate_up(n, l, m).wait())

    def mix_own():
        mix_block(f, mz_send.at[0], bridge).start()
        mix_block(f, mz_send.at[1], pair).start()

    items = (
        *(functools.partial(send_gate_up, 0, r) for r in range(8)), mix_own,
        *(functools.partial(send_down, 0, q) for q in range(n_q)),
        *(functools.partial(send_gate_up, 1, r) for r in range(8)),
        *(functools.partial(send_down, 1, q) for q in range(n_q)))
    inner_plan = (13, 13, 13, 13, 13, 13, 13, 13, 13, 15, 16, 17, 18, 19, 20, 21, 21, 21, 21, 22, 23, 24, 25)
    outer_plan = (9, 10, 11, 12, 13, 13, 13, 13, 13, 14, 15, 16, 17, 18, 19, 20, 20, 20, 20, 21, 22, 23, 25)
    pass_plan = (0, 0, 0, 0, 0, 0, 0, 0, 0, 0, 0, 0, 0, 1, 2, 3, 4, 5, 6, 7, 8, 8, 8)

    def point(p):
        for plan, mask in ((inner_plan, inner), (outer_plan, jnp.logical_not(inner))):
            group = items[plan[p - 1] if p else 0:plan[p]]
            if group:
                @pl.when(mask)
                def _():
                    for item in group:
                        item()
        for r in range(pass_plan[p - 1] if p else 0, pass_plan[p]):
            pass_gate_up(1, r)

    gather_own(0)
    point(0)
    gather_near(0)
    for r in range(8):
        pass_gate_up(0, r)
        point(r + 1)
        if r == 0:
            gather_far(0)
        if r == 3:
            gather_end(0)
    mix_near()
    point(9)
    pass_down(0, 0)
    wait_own(0)
    load_out.wait()
    for r in range(8):
        take_gate_up(0, r)
    hidden_of(0)
    point(10)
    mix_far()
    reduced(0, tuple((k, functools.partial(point, 11 + k)) for k in range(8)))

    squares = jnp.sum(resid[0] * resid[0], axis=-1, keepdims=True)
    for q in range(1, n_q):
        squares = squares + jnp.sum(resid[q] * resid[q], axis=-1, keepdims=True)
    scale = lax.rsqrt(squares * (1.0 / width) + EPS)
    for q in range(n_q):
        for j in range(n_fs):
            cols = slice(j * dc + q * qc, j * dc + (q + 1) * qc)
            xs[1, u, f, :, cols] = (resid[q, :, j * qc:(j + 1) * qc] * scale * gain2[:, cols]).astype(BF16)

    gather_own(1)
    point(19)
    gather_near(1)
    point(20)
    gather_far(1)
    point(21)
    drain_gate_up(0)
    drain_mix()
    gather_end(1)
    point(22)
    drain_down(0)
    drain_steps(0)
    pass_down(1, 0)
    wait_own(1)
    for r in range(8):
        take_gate_up(1, r)
    hidden_of(1)
    reduced(1, ((2, functools.partial(drain_gate_up, 1)), (4, functools.partial(drain_down, 1))))
    drain_steps(1)

    pltpu.make_async_copy(joined, joined, write_sem).wait()


def gathered_call(mesh, args):
    n_fs, n_tp = mesh.shape["fs"], mesh.shape["tp"]
    tokens, mix_heads, _, gate_first = args[:4]
    rows_in, width = tokens.shape
    dc, hidden = gate_first.shape
    heads = mix_heads.shape[1]
    lane, n_q = 128, dc // 128
    n_lane = hidden // lane
    counts = sorted({-(-(j + 1) * n_lane // n_fs) - -(-j * n_lane // n_fs) for j in range(n_fs)})
    most = counts[-1] * lane
    sub, total, qc = rows_in // n_tp, rows_in * n_fs, dc // n_q
    n_x, wide = n_tp // 2, n_fs * qc
    dma = pltpu.SemaphoreType.DMA
    vmem = pl.BlockSpec(memory_space=pltpu.VMEM)
    hbm = pl.BlockSpec(memory_space=pl.ANY)
    lq = (2, n_q)
    return pl.pallas_call(
        functools.partial(gathered, counts, n_fs, n_tp, n_q, lane),
        out_shape=jax.ShapeDtypeStruct((rows_in, width), BF16),
        in_specs=[hbm, hbm, vmem, hbm, hbm, hbm, hbm, vmem, hbm, hbm, hbm],
        out_specs=hbm,
        scratch_shapes=[
            pltpu.VMEM((rows_in, width), BF16),
            pltpu.VMEM((2, 2, width, most), BF16),
            pltpu.VMEM((2, n_q, most, wide), BF16),
            pltpu.VMEM((heads, dc), BF16),
            pltpu.VMEM((2, n_tp, n_fs, sub, width), BF16),
            pltpu.VMEM((n_tp, n_fs, sub, heads), BF16),
            pltpu.VMEM((total, most), BF16),
            pltpu.VMEM((total // 2, wide), F32),
            pltpu.VMEM((*lq, n_tp, n_fs, sub, wide), BF16),
            pltpu.VMEM((*lq, n_x, n_fs, sub, wide), BF16),
            pltpu.VMEM((*lq, n_fs, sub, wide), BF16),
            pltpu.VMEM((*lq, n_fs, sub, wide), BF16),
            pltpu.VMEM((*lq, n_fs, sub, wide), F32),
            pltpu.VMEM((*lq, n_fs, sub, wide), BF16),
            pltpu.VMEM((*lq, sub, wide), BF16),
            pltpu.VMEM((*lq, 2, sub, wide), BF16),
            pltpu.VMEM((*lq, 2, sub, wide), BF16),
            pltpu.VMEM((*lq, sub, wide), BF16),
            pltpu.VMEM((n_q, sub, wide), F32),
            pltpu.VMEM((n_q, sub, wide), BF16),
            pltpu.VMEM((n_q, rows_in, wide), BF16),
            dma, dma, dma, dma((2, 2)), dma(lq), dma,
            dma((2, n_fs)), dma((2, 2, 4)), dma((2,)), dma((2, 2, 4)),
            dma((2, n_fs)), dma((*lq, n_fs)), dma((2,)), dma(lq),
            dma((2,)), dma((2, n_fs, 2)), dma((2,)),
            dma((2,)), dma((2, n_fs, 2)), dma((2,)), dma((2,)), dma((2,)), dma((2,)),
            dma((2,)), dma((n_fs,)), dma((2,)),
            *[dma((2,)), dma(lq)] * 5,
            dma, dma((n_q,)),
        ],
        compiler_params=pltpu.CompilerParams(
            collective_id=0, has_side_effects=True, vmem_limit_bytes=60 * 1024 * 1024),
    )(*args)


def fits(mesh, args):
    tokens, gate = args[0], args[3]
    n_tp = mesh.shape["tp"]
    return (mesh.shape["grp"] == 2 and mesh.shape["fs"] == 4 and n_tp == 4 and tokens.shape[0] % (32 * n_tp) == 0
            and gate.shape[0] % 512 == 0 and gate.shape[1] % 128 == 0)


def solution(mesh):
    n_fs, n_tp = mesh.shape["fs"], mesh.shape["tp"]

    def local(tokens, mix_heads, norm_first, gate_first, up_first, down_first, out_weight,
              norm_second, gate_second, up_second, down_second):
        args = (tokens, mix_heads, norm_first.reshape(1, -1), gate_first, up_first, down_first, out_weight,
                norm_second.reshape(1, -1), gate_second, up_second, down_second)
        if fits(mesh, args):
            return gathered_call(mesh, args)
        rows_in, width = tokens.shape
        total = rows_in * n_fs
        share = total // n_tp
        dc, hidden = gate_first.shape
        heads = mix_heads.shape[1]
        chunk = rows_in // 2
        n_chunks = total // 2 // chunk
        dma = pltpu.SemaphoreType.DMA
        vmem = pl.BlockSpec(memory_space=pltpu.VMEM)
        hbm = pl.BlockSpec(memory_space=pl.ANY)
        return pl.pallas_call(
            functools.partial(kernel, n_fs, n_tp, chunk),
            out_shape=jax.ShapeDtypeStruct((rows_in, width), BF16),
            in_specs=[vmem, vmem, vmem, hbm, hbm, hbm, hbm, vmem, hbm, hbm, hbm],
            out_specs=vmem,
            scratch_shapes=[
                pltpu.VMEM(gate_first.shape, BF16),
                pltpu.VMEM(up_first.shape, BF16),
                pltpu.VMEM(down_first.shape, BF16),
                pltpu.VMEM(out_weight.shape, BF16),
                pltpu.VMEM(gate_second.shape, BF16),
                pltpu.VMEM(up_second.shape, BF16),
                pltpu.VMEM(down_second.shape, BF16),
                pltpu.VMEM((total, dc), BF16),
                pltpu.VMEM((total, dc), BF16),
                pltpu.VMEM((total, heads), BF16),
                pltpu.VMEM((2, total, hidden), F32),
                pltpu.VMEM((2, total, hidden), BF16),
                pltpu.VMEM((2, total, hidden), BF16),
                pltpu.VMEM((2, total, hidden), BF16),
                pltpu.VMEM((total, hidden), BF16),
                pltpu.VMEM((total, hidden), BF16),
                pltpu.VMEM((total, dc), BF16),
                pltpu.VMEM((n_tp, share, dc), BF16),
                pltpu.VMEM((n_tp, share, dc), BF16),
                pltpu.VMEM((share, dc), F32),
                pltpu.VMEM((n_fs, 8, rows_in), F32),
                pltpu.VMEM((n_fs, 8, share), F32),
                pltpu.VMEM((share, dc), BF16),
                pltpu.VMEM((rows_in, width), BF16),
                dma((7,)), dma((n_fs,)), dma((n_fs,)), dma((n_fs,)), dma((n_fs,)), dma((n_fs,)), dma((n_fs,)),
                dma((n_fs, 2)), dma((n_fs,)),
                dma((2, 2, n_chunks)), dma((2, 2, n_chunks)), dma((2, 2, n_chunks)), dma((2, 2, n_chunks)),
                dma((2, n_tp)), dma((2, n_tp)),
                dma((n_fs,)), dma((n_fs,)), dma((n_tp,)), dma((n_tp,)), dma((n_tp,)), dma((n_tp,)),
                dma((n_tp,)), dma((n_fs,)), dma((n_fs,)), dma((n_fs,)),
            ],
            compiler_params=pltpu.CompilerParams(
                collective_id=0, has_side_effects=True, vmem_limit_bytes=60 * 1024 * 1024),
        )(*args)

    in_specs = (
        P(("grp", "fs"), None),
        P(("grp", "fs"), "tp"),
        P(),
        P("fs", "tp"),
        P("fs", "tp"),
        P("tp", "fs"),
        P("tp", "fs"),
        P(),
        P("fs", "tp"),
        P("fs", "tp"),
        P("tp", "fs"),
    )
    return jax.shard_map(local, mesh=mesh, in_specs=in_specs, out_specs=P(("grp", "fs"), None), check_vma=False)
```

```python
import functools

import jax
import jax.numpy as jnp
from jax import lax
from jax.experimental import pallas as pl
from jax.experimental.pallas import tpu as pltpu
from jax.sharding import PartitionSpec as P

EPS = 0.1
MESH = pl.DeviceIdType.MESH
BF16 = jnp.bfloat16
F32 = jnp.float32


def loop(count, body):
    def step(i, carry):
        body(i)
        return carry

    lax.fori_loop(0, count, step, 0)


def kernel(n_fs, n_tp, chunk,
           tok, mix, gain1, wg1, wu1, wd1, wo, gain2, wg2, wu2, wd2,
           out,
           vg1, vu1, vd1, vo, vg2, vu2, vd2,
           raw, nb2, mixed, grads, sums, in1, in2, hid1, hid2,
           terms, got1, got2, resid, squares1, squares, done_rows, joined,
           wsem, p0_send, p0_recv, fw_send, fw_recv, s1_send, s1_recv, mix_send, mix_recv,
           rs_send, rs_recv, ag_send, ag_recv, tp_send, tp_recv,
           sq_send, sq_recv, nrm_send, nrm_recv, nfw_send, nfw_recv,
           out_send, out_recv, ofw_send, ofw_recv):
    f, t = lax.axis_index("fs"), lax.axis_index("tp")
    rows_in, width = tok.shape
    total = rows_in * n_fs
    share = total // n_tp
    half = total // 2
    n_chunks = half // chunk
    dc = width // n_fs

    weights = ((wg1, vg1), (wu1, vu1), (wd1, vd1), (wo, vo), (wg2, vg2), (wu2, vu2), (wd2, vd2))
    loads = [pltpu.make_async_copy(a, b, wsem.at[i]) for i, (a, b) in enumerate(weights)]
    for load in loads:
        load.start()

    barrier = pltpu.get_barrier_semaphore()

    def greet(i):
        pf, pt = i // n_tp, i % n_tp

        @pl.when(jnp.logical_or(pf != f, pt != t))
        def _():
            pl.semaphore_signal(barrier, inc=1, device_id={"fs": pf, "tp": pt}, device_id_type=MESH)

    loop(n_fs * n_tp, greet)

    def cols(j):
        return pl.ds(pl.multiple_of(j * dc, dc), dc)

    def block(j, size):
        return pl.ds(pl.multiple_of(j * size, size), size)

    def remote(src, dst, send, recv, **where):
        return pltpu.make_async_remote_copy(
            src_ref=src, dst_ref=dst, send_sem=send, recv_sem=recv,
            device_id=where, device_id_type=MESH)

    c_own = t % 2
    partner = t + 1 - 2 * c_own
    half_in = rows_in // 2
    n_pairs = n_tp // 2

    def squares_of(x):
        own = jnp.sum(x * x, axis=-1, keepdims=True)
        return jnp.transpose(jnp.broadcast_to(own, (x.shape[0], 128)))[0:8, :]

    def scale_of(summed):
        column = jnp.transpose(jnp.broadcast_to(summed[0:1, :], (128, summed.shape[1])))[:, 0:1]
        return lax.rsqrt(column * (1.0 / width) + EPS)

    def piece_of(slot):
        return pl.ds(pl.multiple_of(slot * rows_in + c_own * half_in, half_in), half_in)

    def p0_copy(j, slot):
        return remote(tok.at[block(c_own, half_in), cols(j)], raw.at[piece_of(slot), :],
                      p0_send.at[j], p0_recv.at[slot], fs=j)

    def fw_copy(slot):
        place = raw.at[piece_of(slot), :]
        return remote(place, place, fw_send.at[slot], fw_recv.at[slot], tp=partner)

    def s1_copy(j, slot):
        return remote(squares1.at[f], squares1.at[slot], s1_send.at[j], s1_recv.at[slot], fs=j)

    def sq_copy(j, slot):
        return remote(squares.at[f], squares.at[slot], sq_send.at[j], sq_recv.at[slot], fs=j)

    def mix_copy(slot, side, where):
        place = mixed.at[block(slot, rows_in), :]
        return remote(place, place, mix_send.at[slot, side], mix_recv.at[slot], fs=where)

    mixed[block(f, rows_in), :] = mix[...]
    pl.semaphore_wait(barrier, n_fs * n_tp - 1)

    def p0_start(i):
        p0_copy((f + 1 + i) % n_fs, f).start()

    loop(n_fs - 1, p0_start)
    squares1[f] = squares_of(tok[...].astype(F32))

    def s1_start(i):
        s1_copy((f + 1 + i) % n_fs, f).start()

    loop(n_fs - 1, s1_start)

    @pl.when(f < n_fs - 1)
    def _():
        mix_copy(f, 0, f + 1).start()

    @pl.when(f > 0)
    def _():
        mix_copy(f, 1, f - 1).start()

    raw[block(f, rows_in), :] = tok[:, cols(f)]

    def gates_one(j):
        rows = block(j, rows_in)
        x = (raw[rows, :].astype(F32) * scale_of(squares1[j]) * gain1[:, cols(f)]).astype(BF16)
        grads[0, rows, :] = jnp.dot(x, vg1[...], preferred_element_type=F32)
        grads[1, rows, :] = jnp.dot(x, vu1[...], preferred_element_type=F32)

    def side_of(side):
        hops = jnp.where(side == 0, n_fs - 1 - f, f)
        toward = jnp.where(side == 0, f - 1, f + 1)
        away = jnp.where(side == 0, f + 1, f - 1)
        return hops, toward, away

    near = jnp.where(2 * f >= n_fs, 0, 1)

    def chain(layer, arrived, hid, with_mix):
        def rows_of(side, c):
            return pl.ds(pl.multiple_of(side * half + c * chunk, chunk), chunk)

        def rs_copy(side, c, where):
            rows = rows_of(side, c)
            return remote(sums.at[:, rows, :], arrived.at[:, rows, :],
                          rs_send.at[layer, side, c], rs_recv.at[layer, side, c], fs=where)

        def ag_copy(side, c, where):
            rows = rows_of(side, c)
            return remote(hid.at[rows, :], hid.at[rows, :],
                          ag_send.at[layer, side, c], ag_recv.at[layer, side, c], fs=where)

        for side in (0, 1):
            hops, toward, away = side_of(side)

            @pl.when(hops == 0)
            def _():
                def first(c):
                    rows = rows_of(side, c)
                    sums[:, rows, :] = grads[:, rows, :].astype(BF16)
                    rs_copy(side, c, toward).start()

                loop(n_chunks, first)

        def step(s):
            for k in (0, 1):
                side = near if k == 0 else 1 - near
                hops, toward, away = side_of(side)
                c = s - hops

                @pl.when(jnp.logical_and(hops > 0, jnp.logical_and(c >= 0, c < n_chunks)))
                def _():
                    rows = rows_of(side, c)
                    rs_copy(side, c, f).wait_recv()

                    @pl.when(hops < n_fs - 1)
                    def _():
                        sums[:, rows, :] = (grads[:, rows, :] + arrived[:, rows, :].astype(F32)).astype(BF16)
                        rs_copy(side, c, toward).start()

                    @pl.when(hops == n_fs - 1)
                    def _():
                        g = grads[0, rows, :] + arrived[0, rows, :].astype(F32)
                        v = grads[1, rows, :] + arrived[1, rows, :].astype(F32)
                        hid[rows, :] = (g / (1.0 + jnp.exp(-g)) * v).astype(BF16)
                        ag_copy(side, c, away).start()

            if with_mix:
                @pl.when(jnp.logical_and(s > 0, s < n_fs))
                def _():
                    low, high = f - s, f + s

                    @pl.when(low >= 0)
                    def _():
                        mix_copy(low, 0, f).wait_recv()

                        @pl.when(f < n_fs - 1)
                        def _():
                            mix_copy(low, 0, f + 1).start()

                    @pl.when(high < n_fs)
                    def _():
                        mix_copy(high, 1, f).wait_recv()

                        @pl.when(f > 0)
                        def _():
                            mix_copy(high, 1, f - 1).start()

        loop(n_chunks + n_fs - 1, step)

        def relay(c):
            for k in (0, 1):
                side = 1 - near if k == 0 else near
                hops, toward, away = side_of(side)

                @pl.when(hops < n_fs - 1)
                def _():
                    ag_copy(side, c, f).wait_recv()

                    @pl.when(hops > 0)
                    def _():
                        ag_copy(side, c, away).start()

        def drain(c):
            for side in (0, 1):
                hops, toward, away = side_of(side)

                @pl.when(hops < n_fs - 1)
                def _():
                    rs_copy(side, c, f).wait_send()

                @pl.when(hops > 0)
                def _():
                    ag_copy(side, c, f).wait_send()

        return relay, lambda: loop(n_chunks, drain)

    def tp_copy(layer, j, slot, got):
        return remote(terms.at[block(j, share), :], got.at[slot],
                      tp_send.at[layer, j], tp_recv.at[layer, slot], tp=j)

    def down(layer, relay, hid, vd, got, with_mix):
        per_block = n_chunks // n_pairs

        def piece(b):
            def inner(i):
                relay(b * per_block + i)

            loop(per_block, inner)
            for side in (0, 1):
                j = side * n_pairs + b
                rows = block(j, share)
                value = 0.5 * jnp.dot(hid[rows, :], vd[...], preferred_element_type=F32)
                if with_mix:
                    value = value + jnp.dot(mixed[rows, :], vo[...], preferred_element_type=F32)
                terms[rows, :] = value.astype(BF16)

                @pl.when(j != t)
                def _():
                    tp_copy(layer, j, t, got).start()

        loop(n_pairs, piece)

    def reduce_tp(layer, got, start_value):
        resid[...] = start_value + terms[block(t, share), :].astype(F32)

        def add(i):
            j = (t + 1 + i) % n_tp
            tp_copy(layer, j, j, got).wait_recv()
            resid[...] = resid[...] + got[j].astype(F32)

        loop(n_tp - 1, add)

        def drain(i):
            j = (t + 1 + i) % n_tp
            tp_copy(layer, j, t, got).wait_send()

        loop(n_tp - 1, drain)

    loads[0].wait()
    loads[1].wait()
    gates_one(f)

    def pass_on(i):
        j = (f + 1 + i) % n_fs
        p0_copy(j, j).wait_recv()
        fw_copy(j).start()

    loop(n_fs - 1, pass_on)

    def other_rows(i):
        j = (f + 1 + i) % n_fs
        s1_copy(j, j).wait_recv()
        fw_in(j).wait_recv()
        gates_one(j)

    def fw_in(slot):
        start = pl.multiple_of(slot * rows_in + (1 - c_own) * half_in, half_in)
        place = raw.at[pl.ds(start, half_in), :]
        return remote(place, place, fw_send.at[slot], fw_recv.at[slot], tp=partner)

    loop(n_fs - 1, other_rows)
    relay_one, drain_one = chain(0, in1, hid1, True)
    loads[2].wait()
    loads[3].wait()
    down(0, relay_one, hid1, vd1, got1, True)
    reduce_tp(0, got1, raw[block(t, share), :].astype(F32))

    squares[f] = squares_of(resid[...])

    def sq_start(i):
        sq_copy((f + 1 + i) % n_fs, f).start()

    def sq_wait(i):
        j = (f + 1 + i) % n_fs
        sq_copy(j, j).wait_recv()

    loop(n_fs - 1, sq_start)
    drain_one()
    loop(n_fs - 1, sq_wait)
    summed = squares[0]
    for j in range(1, n_fs):
        summed = summed + squares[j]
    nb2[block(t, share), :] = (resid[...] * scale_of(summed) * gain2[:, cols(f)]).astype(BF16)

    def nrm_copy(j, slot):
        place = nb2.at[block(slot, share), :]
        return remote(place, place, nrm_send.at[j], nrm_recv.at[slot], tp=j)

    def nfw_copy(slot):
        place = nb2.at[block(slot, share), :]
        return remote(place, place, nfw_send.at[slot], nfw_recv.at[slot], tp=partner)

    def same_core(i):
        return (t + 2 + 2 * i) % n_tp

    def nrm_start(i):
        nrm_copy(same_core(i), t).start()

    loop(n_pairs - 1, nrm_start)
    nfw_copy(t).start()
    loads[4].wait()
    loads[5].wait()

    def gates_two(j):
        rows = block(j, share)
        x = nb2[rows, :]
        grads[0, rows, :] = jnp.dot(x, vg2[...], preferred_element_type=F32)
        grads[1, rows, :] = jnp.dot(x, vu2[...], preferred_element_type=F32)

    gates_two(t)
    nfw_copy(partner).wait_recv()
    gates_two(partner)

    def nrm_pass(i):
        j = same_core(i)
        nrm_copy(j, j).wait_recv()
        nfw_copy(j).start()
        gates_two(j)

    loop(n_pairs - 1, nrm_pass)

    def nrm_last(i):
        j = (partner + 2 + 2 * i) % n_tp
        nfw_copy(j).wait_recv()
        gates_two(j)

    loop(n_pairs - 1, nrm_last)
    relay_two, drain_two = chain(1, in2, hid2, False)
    loads[6].wait()
    down(1, relay_two, hid2, vd2, got2, False)
    reduce_tp(1, got2, resid[...])
    done_rows[...] = resid[...].astype(BF16)

    def out_copy(j, slot):
        return remote(done_rows, joined.at[:, cols(slot)], out_send.at[j], out_recv.at[slot], fs=t, tp=j)

    def ofw_copy(slot):
        place = joined.at[:, cols(slot)]
        return remote(place, place, ofw_send.at[slot], ofw_recv.at[slot], tp=partner)

    def out_start(i):
        j = c_own + 2 * i

        @pl.when(jnp.logical_or(f != t, j != t))
        def _():
            out_copy(j, f).start()

    loop(n_pairs, out_start)

    @pl.when(f == t)
    def _():
        joined[:, cols(f)] = done_rows[...]

    takes = c_own == f % 2

    @pl.when(takes)
    def _():
        def take(i):
            j = (f + i) % n_fs

            @pl.when(jnp.logical_or(f != t, j != f))
            def _():
                out_copy(t, j).wait_recv()

            ofw_copy(j).start()

        loop(n_fs, take)

    @pl.when(jnp.logical_not(takes))
    def _():
        def take(i):
            ofw_copy((f + i) % n_fs).wait_recv()

        loop(n_fs, take)

    out[...] = joined[...]

    drain_two()

    def last_fs(i):
        j = (f + 1 + i) % n_fs
        p0_copy(j, f).wait_send()
        fw_copy(j).wait_send()
        s1_copy(j, f).wait_send()
        sq_copy(j, f).wait_send()

    loop(n_fs - 1, last_fs)

    def last_mix(j):
        @pl.when(jnp.logical_and(j <= f, f < n_fs - 1))
        def _():
            mix_copy(j, 0, f).wait_send()

        @pl.when(jnp.logical_and(j >= f, f > 0))
        def _():
            mix_copy(j, 1, f).wait_send()

        @pl.when(takes)
        def _():
            ofw_copy(j).wait_send()

    loop(n_fs, last_mix)

    def last_nrm(i):
        nrm_copy(same_core(i), t).wait_send()

    loop(n_pairs - 1, last_nrm)

    def last_out(i):
        j = c_own + 2 * i
        nfw_copy(j).wait_send()

        @pl.when(jnp.logical_or(f != t, j != t))
        def _():
            out_copy(j, f).wait_send()

    loop(n_pairs, last_out)


def by_count(counts, value, body):
    for n in counts:
        if len(counts) == 1:
            body(n)
        else:
            pl.when(value == n)(functools.partial(body, n))


def gathered(counts, n_fs, n_tp, n_q, lane,
             tok, mix, gain1, wg1, wu1, wd1, wo, gain2, wg2, wu2, wd2,
             out,
             rows_of_me, wgu, wdb, wob, xs, mixed, hid, acc, part, r1, s1, r2, full, zs, rp, rr, zf, rf, rg, resid, done, joined,
             tok_sem, mix_sem, write_sem, wl_sem, dl_sem, wo_sem,
             wz_send, wz_recv, wy_send, wy_recv, dz_send, dz_recv, dy_send, dy_recv,
             ag_send, ag_recv, agr_send, ax_send, ax_recv, ad_send, ad_recv, af_send, af_recv,
             mz_send, mz_recv, mr_send,
             r1_send, r1_recv, r2_send, r2_recv, rp_send, rp_recv, rr_send, rr_recv, rf_send, rf_recv, rg_send, rg_recv,
             o_send, o_recv):
    g, f, t = lax.axis_index("grp"), lax.axis_index("fs"), lax.axis_index("tp")
    rows_in, width = tok.shape
    dc, hidden = wg1.shape
    n_x = n_tp // 2
    core, x = t % 2, t // 2
    sub = rows_in // n_tp
    unit = n_fs * sub
    u = core * n_x + x
    u_x = core * n_x + 1 - x
    u_pair = (1 - core) * n_x + x
    u_diag = (1 - core) * n_x + 1 - x
    t_x = (t + 2) % n_tp
    t_pair = t + 1 - 2 * core
    t_diag = (t_pair + 2) % n_tp
    pair = f + 1 - 2 * (f % 2)
    far0 = jnp.where(f < 2, 2, 0)
    inner = jnp.logical_or(f == 1, f == 2)
    bridge = jnp.where(f < 2, 2, 1)
    others = (jnp.where(f < 2, n_fs - 1, 0), bridge, pair)
    n_k = 4
    piece = dc // (2 * n_k)
    qc = dc // n_q
    n_lane = hidden // lane
    most = max(counts)
    gate_up = ((wg1, wu1), (wg2, wu2))
    downs = (wd1, wd2)

    def first(j):
        return (j * n_lane + (1 - core) * (n_fs - 1)) // n_fs

    def count(j):
        return first(j + 1) - first(j)

    mine = count(f)

    def at(i, size):
        return pl.ds(pl.multiple_of(i * size, size), size)

    def remote(src, dst, send, recv, **where):
        return pltpu.make_async_remote_copy(
            src_ref=src, dst_ref=dst, send_sem=send, recv_sem=recv,
            device_id=where, device_id_type=MESH)

    def load_gate_up(n, l, m):
        cols = pl.ds(pl.multiple_of(first(f) * lane, lane), n * lane)
        return pltpu.make_async_copy(
            gate_up[l][m].at[:, cols], wgu.at[l, m, at(f, dc), pl.ds(0, n * lane)], wl_sem.at[l, m])

    def load_down(n, l, q):
        rows = pl.ds(pl.multiple_of(first(f) * lane, lane), n * lane)
        return pltpu.make_async_copy(
            downs[l].at[rows, at(q, qc)], wdb.at[l, q, pl.ds(0, n * lane), at(f, qc)], dl_sem.at[l, q])

    def start_loads(n):
        for l in (0, 1):
            for m in (0, 1):
                load_gate_up(n, l, m).start()
            for q in range(n_q):
                load_down(n, l, q).start()
        if n < most:
            rest = pl.ds(n * lane, (most - n) * lane)
            wgu[:, :, :, rest] = jnp.zeros((2, 2, width, (most - n) * lane), BF16)
            wdb[:, :, rest, :] = jnp.zeros((2, n_q, (most - n) * lane, n_fs * qc), BF16)

    barrier = pltpu.get_barrier_semaphore()
    for i in range(n_fs - 1):
        pl.semaphore_signal(barrier, inc=1, device_id={"fs": others[i]}, device_id_type=MESH)
    pl.semaphore_signal(barrier, inc=1, device_id={"grp": 1 - g}, device_id_type=MESH)
    for j in (t_x, t_pair, t_diag):
        pl.semaphore_signal(barrier, inc=1, device_id={"tp": j}, device_id_type=MESH)

    load_tok = pltpu.make_async_copy(tok, rows_of_me, tok_sem)
    load_tok.start()
    load_mix = [pltpu.make_async_copy(
        mix.at[j * sub:(j + 1) * sub, :], mixed.at[(j % 2) * n_x + j // 2, f], mix_sem) for j in range(n_tp)]
    for load in load_mix:
        load.start()
    by_count(counts, mine, start_loads)
    load_out = pltpu.make_async_copy(wo, wob, wo_sem)
    load_out.start()

    def normed(values, gain):
        squares = jnp.sum(values * values, axis=-1, keepdims=True)
        return values * lax.rsqrt(squares * (1.0 / width) + EPS) * gain

    load_tok.wait()
    own = rows_of_me[at(t, sub), :].astype(F32)
    xs[0, u, f] = normed(own, gain1[...]).astype(BF16)
    for j in range(n_tp):
        @pl.when(j != t)
        def _():
            rows = rows_of_me[j * sub:(j + 1) * sub, :].astype(F32)
            xs[0, (j % 2) * n_x + j // 2, f] = normed(rows, gain1[...]).astype(BF16)
    for q in range(n_q):
        for j in range(n_fs):
            resid[q, :, j * qc:(j + 1) * qc] = own[:, j * dc + q * qc:j * dc + (q + 1) * qc]
    pltpu.make_async_copy(mixed.at[:, f], mixed.at[:, f], mix_sem).wait()
    pl.semaphore_wait(barrier, n_fs - 1 + 1 + n_tp - 1)

    def send_one(n, l, m, k, j):
        cols = pl.ds(pl.multiple_of(first(j) * lane, lane), n * lane)
        remote(gate_up[l][m].at[at(n_k * g + k, piece), cols],
               wgu.at[l, m, at(n_k * (2 * f + g) + k, piece), pl.ds(0, n * lane)],
               wz_send.at[l, j], wz_recv.at[l, m, k], fs=j).start()

    def send_gate_up(l, r, where=others):
        for j in where:
            by_count(counts, count(j), lambda n, j=j: send_one(n, l, r % 2, r // 2, j))

    def gate_up_y(n, l, m, k, j):
        place = wgu.at[l, m, at(n_k * (2 * j + g) + k, piece), pl.ds(0, n * lane)]
        return remote(place, place, wy_send.at[l], wy_recv.at[l, m, k], grp=1 - g)

    def all_pieces(n, l, m, k, send, recv):
        place = wgu.at[l, m, pl.ds(0, len(others) * piece), pl.ds(0, n * lane)]
        return remote(place, place, send, recv, grp=1 - g)

    def pass_gate_up(l, r):
        m, k = r % 2, r // 2

        def go(n):
            all_pieces(n, l, m, k, wz_send.at[l, pair], wz_recv.at[l, m, k]).wait_recv()
            for j in others:
                gate_up_y(n, l, m, k, j).start()

        by_count(counts, mine, go)

    def take_gate_up(l, r):
        m, k = r % 2, r // 2
        by_count(counts, mine, lambda n: all_pieces(n, l, m, k, wy_send.at[l], wy_recv.at[l, m, k]).wait_recv())

    def down_part(n, l, q, j, side):
        size = n * lane // 2
        return wdb.at[l, q, at(side, size), at(j, qc)]

    def send_down(l, q, where=others):
        for j in where:
            def go(n, j=j):
                size = n * lane // 2
                rows = pl.ds(pl.multiple_of(first(j) * lane + g * size, lane // 2), size)
                remote(downs[l].at[rows, at(q, qc)], down_part(n, l, q, f, g),
                       dz_send.at[l, j], dz_recv.at[l, q, f], fs=j).start()

            by_count(counts, count(j), go)

    def down_y(n, l, q, j):
        place = down_part(n, l, q, j, g)
        return remote(place, place, dy_send.at[l], dy_recv.at[l, q], grp=1 - g)

    def all_downs(n, l, q, send, recv):
        place = wdb.at[l, q, pl.ds(0, n * lane // 2), pl.ds(0, len(others) * qc)]
        return remote(place, place, send, recv, grp=1 - g)

    def z_block(l, j, h, send, where):
        place = xs.at[l, u, j, at(h, sub // 2)]
        return remote(place, place, send, ag_recv.at[l, j, h], fs=where)

    def x_block(l, j, who, h):
        place = xs.at[l, who, j, at(h, sub // 2)]
        return remote(place, place, ax_send.at[l], ax_recv.at[l, j, h], tp=t_x)

    def pair_block(l, j, who, h):
        place = xs.at[l, who, j, at(h, sub // 2)]
        return remote(place, place, ad_send.at[l], ad_recv.at[l], tp=t_pair)

    def diag_block(l, j, who, h):
        place = xs.at[l, who, j, at(h, sub // 2)]
        return remote(place, place, af_send.at[l], af_recv.at[l], tp=t_pair)

    def pass_rows(l, j, h):
        x_block(l, j, u, h).start()
        pair_block(l, j, u, h).start()

    def gather_own(l):
        for h in (0, 1):
            z_block(l, f, h, ag_send.at[l], bridge).start()
        for h in (0, 1):
            z_block(l, f, h, ag_send.at[l], pair).start()
            if l == 1:
                pass_rows(l, f, h)

    def gather_near(l):
        for h in (0, 1):
            for k in (0, 1):
                @pl.when(inner)
                def _():
                    j = far0 + k
                    z_block(l, j, h, agr_send.at[l], j).wait_recv()
                    z_block(l, j, h, agr_send.at[l], pair).start()
                    pass_rows(l, j, h)

        for h in (0, 1):
            z_block(l, pair, h, ag_send.at[l], pair).wait_recv()
            pass_rows(l, pair, h)

    def gather_far(l):
        for h in (0, 1):
            for k in (0, 1):
                @pl.when(jnp.logical_not(inner))
                def _():
                    j = far0 + k
                    z_block(l, j, h, agr_send.at[l], j).wait_recv()
                    pass_rows(l, j, h)

    def gather_end(l):
        blocks = [(j, h) for j in (far0, far0 + 1, pair) for h in (0, 1)]
        if l == 1:
            blocks = [(f, 0), (f, 1)] + blocks
        for j, h in blocks:
            x_block(l, j, u_x, h).wait_recv()
            diag_block(l, j, u_x, h).start()
        rows = xs.at[l, 0, pl.ds(0, len(blocks) // 2)]
        remote(rows, rows, ad_send.at[l], ad_recv.at[l], tp=t_pair).wait_recv()
        remote(rows, rows, af_send.at[l], af_recv.at[l], tp=t_pair).wait_recv()

    def mix_block(j, send, where):
        place = mixed.at[:, j]
        return remote(place, place, send, mz_recv.at[j], fs=where)

    def mix_near():
        @pl.when(inner)
        def _():
            for k in (0, 1):
                j = far0 + k
                mix_block(j, mr_send.at[k], j).wait_recv()
                mix_block(j, mr_send.at[k], pair).start()

    def mix_far():
        @pl.when(jnp.logical_not(inner))
        def _():
            for k in (0, 1):
                mix_block(far0 + k, mr_send.at[k], far0 + k).wait_recv()

        mix_block(pair, mz_send.at[1], pair).wait_recv()

    def hidden_of(l):
        def step(i):
            rows = xs[l, at(i, n_x)].reshape(n_x * unit, width)
            gate = jnp.dot(rows, wgu[l, 0], preferred_element_type=F32)
            value = jnp.dot(rows, wgu[l, 1], preferred_element_type=F32)
            hid[at(i, n_x * unit), :] = (gate / (1.0 + jnp.exp(-gate)) * value).astype(BF16)

        loop(2, step)

    def s1_copy(l, q):
        return remote(part.at[l, q, at(1 - core, n_x)], r1.at[l, q], r1_send.at[l], r1_recv.at[l, q], tp=t_pair)

    def s2_copy(l, q):
        return remote(s1.at[l, q], r2.at[l, q], r2_send.at[l], r2_recv.at[l, q], tp=t_x)

    def pair_copy(l, q):
        return remote(zs.at[l, q, pair], rp.at[l, q], rp_send.at[l], rp_recv.at[l, q], fs=pair)

    def relay_copy(q):
        return remote(zs.at[0, q, pl.ds(far0, 2)], rr.at[q], rr_send, rr_recv.at[q], fs=pair)

    def far_copy(q, k, where):
        return remote(zf.at[q, k], rf.at[0, q], rf_send.at[0], rf_recv.at[0, q], fs=where)

    def straight(q, k, where):
        return remote(zs.at[1, q, far0 + k], rg.at[q], rg_send, rg_recv.at[q], fs=where)

    def straight_inner(q, k, where):
        return remote(zs.at[1, q, far0 + k], rf.at[1, q], rf_send.at[1], rf_recv.at[1, q], fs=where)

    def out_copy(q, where, who):
        return remote(done.at[q], joined.at[q, at(who, sub)], o_send, o_recv.at[q], tp=where)

    def pass_down(l, q):
        def go(n):
            for j in others:
                place = down_part(n, l, q, j, g)
                remote(place, place, dz_send.at[l, j], dz_recv.at[l, q, j], fs=j).wait_recv()
                down_y(n, l, q, j).start()

        by_count(counts, mine, go)

    def write_copy(q, j):
        return pltpu.make_async_copy(
            joined.at[q, :, at(j, qc)], out.at[:, pl.ds(pl.multiple_of(j * dc + q * qc, qc), qc)], write_sem)

    def reduced(l, hooks):
        def multiply(q):
            @pl.when(q < n_q - 1)
            def _():
                pass_down(l, q + 1)

            def ready(n):
                all_downs(n, l, q, dy_send.at[l], dy_recv.at[l, q]).wait_recv()
                load_down(n, l, q).wait()

            by_count(counts, mine, ready)

            def side(i):
                c = (1 - core) * (1 - i) + core * i
                value = 0.5 * jnp.dot(hid[at(c, n_x * unit), :], wdb[l, q], preferred_element_type=F32)
                if l == 0:
                    acc[...] = value
                    heads = mixed[at(c, n_x)].reshape(n_x * unit, mixed.shape[-1])
                    acc[:, at(f, qc)] = acc[:, at(f, qc)] + jnp.dot(
                        heads, wob[:, at(q, qc)], preferred_element_type=F32)
                    value = acc[...]
                part[l, q, at(c, n_x)] = value.astype(BF16).reshape(n_x, n_fs, sub, n_fs * qc)

                @pl.when(i == 0)
                def _():
                    s1_copy(l, q).start()

            loop(2, side)

        def across(q):
            s1_copy(l, q).wait_recv()
            s1[l, q] = (part[l, q, u_x].astype(F32) + r1[l, q, 1 - x].astype(F32)).astype(BF16)
            s2_copy(l, q).start()

        def along(q):
            s2_copy(l, q).wait_recv()
            value = part[l, q, u].astype(F32) + r1[l, q, x].astype(F32) + r2[l, q].astype(F32)
            full[l, q] = value
            zs[l, q] = value.astype(BF16)

            if l == 0:
                pl.when(jnp.logical_not(inner))(lambda: relay_copy(q).start())
            else:
                @pl.when(inner)
                def _():
                    for k in (0, 1):
                        straight_inner(q, k, far0 + k).start()

                @pl.when(jnp.logical_not(inner))
                def _():
                    for k in (0, 1):
                        straight(q, k, far0 + k).start()

            pair_copy(l, q).start()

        def relay(q):
            @pl.when(inner)
            def _():
                relay_copy(q).wait_recv()
                for k in (0, 1):
                    zf[q, k] = (full[0, q, far0 + k] + rr[q, k].astype(F32)).astype(BF16)
                    far_copy(q, k, far0 + k).start()

        def finish(q):
            pair_copy(l, q).wait_recv()
            value = full[l, q, f] + rp[l, q].astype(F32)
            if l == 0:
                far_copy(q, 0, far0).wait_recv()
            else:
                straight_inner(q, 0, far0).wait_recv()
                straight(q, 0, far0).wait_recv()
                value = value + rg[q].astype(F32)
            value = resid[q] + (value + rf[l, q].astype(F32))
            if l == 0:
                resid[q] = value
            else:
                done[q] = value.astype(BF16)
                joined[q, at(t, sub)] = value.astype(BF16)
                for where in (t_x, t_diag, t_pair):
                    out_copy(q, where, t).start()

        def write(q):
            rows = joined.at[q, pl.ds(0, (n_tp - 1) * sub)]
            remote(rows, rows, o_send, o_recv.at[q], tp=t_pair).wait_recv()
            for j in range(n_fs):
                write_copy(q, j).start()

        stages = [(multiply, 0), (across, 0), (along, 1)]
        stages += [(relay, 2), (finish, 4)] if l == 0 else [(finish, 2), (write, 3)]

        def step(s):
            for stage, lag in stages:
                @pl.when(jnp.logical_and(s >= lag, s < n_q + lag))
                def _():
                    stage(s - lag)

            for when, hook in hooks:
                pl.when(s == when)(hook)

        loop(n_q + stages[-1][1], step)

    def sent(ref, sem):
        remote(ref, ref, sem, ag_recv.at[0, 0, 0], tp=t_pair).wait_send()

    def drain_gate_up(l):
        for j in others:
            by_count(counts, count(j), lambda n, j=j: sent(
                wgu.at[l, 0, pl.ds(0, dc), pl.ds(0, n * lane)], wz_send.at[l, j]))
        by_count(counts, mine, lambda n: sent(
            wgu.at[l, 0, pl.ds(0, len(others) * dc), pl.ds(0, n * lane)], wy_send.at[l]))
        sent(xs.at[l, 0, pl.ds(0, 2)], ag_send.at[l])
        pl.when(inner)(lambda: sent(xs.at[l, 0, pl.ds(0, 2)], agr_send.at[l]))
        rows = xs.at[l, 0, pl.ds(0, 4 if l == 1 else 3)]
        for sem in (ax_send, ad_send, af_send):
            sent(rows, sem.at[l])

    def drain_mix():
        mix_block(f, mz_send.at[0], bridge).wait_send()
        mix_block(f, mz_send.at[1], pair).wait_send()

        @pl.when(inner)
        def _():
            for k in (0, 1):
                mix_block(far0 + k, mr_send.at[k], pair).wait_send()

    def drain_down(l):
        for j in others:
            by_count(counts, count(j), lambda n, j=j: sent(
                wdb.at[l, 0, pl.ds(0, n * lane // 2)], dz_send.at[l, j]))
        by_count(counts, mine, lambda n: sent(
            wdb.at[l, pl.ds(0, len(others)), pl.ds(0, n * lane // 2)], dy_send.at[l]))

    def drain_steps(l):
        sent(part.at[l, :, pl.ds(0, n_x)], r1_send.at[l])
        sent(s1.at[l], r2_send.at[l])
        sent(zs.at[l, 0], rp_send.at[l])
        pl.when(inner)(lambda: sent(zs.at[l, pl.ds(0, 2)], rf_send.at[l]))
        pl.when(jnp.logical_not(inner))(lambda: sent(zs.at[l, pl.ds(0, 2)], rg_send if l else rr_send))
        if l == 1:
            sent(joined.at[:, pl.ds(0, (n_tp - 1) * sub)], o_send)

    def wait_own(l):
        for m in (0, 1):
            by_count(counts, mine, lambda n, m=m: load_gate_up(n, l, m).wait())

    cross, near = others[:2], others[2:]

    def mix_to(where):
        if where is not near:
            mix_block(f, mz_send.at[0], bridge).start()
        if where is not cross:
            mix_block(f, mz_send.at[1], pair).start()

    items = [
        *(functools.partial(send_gate_up, 0, r) for r in range(8)),
        *(functools.partial(send_down, 0, q) for q in range(n_q)),
        *(functools.partial(send_gate_up, 1, r) for r in range(8)),
        *(functools.partial(send_down, 1, q) for q in range(n_q))]
    items.insert(5, mix_to)
    plans = (
        (inner, cross, (13, 13, 13, 13, 13, 13, 13, 13, 13, 15, 16, 17, 18, 19, 20, 21, 21, 21, 21, 22, 23, 24, 25)),
        (inner, near, (13, 13, 13, 13, 13, 13, 13, 13, 13, 15, 16, 17, 18, 19, 20, 21, 21, 21, 21, 22, 23, 24, 25)),
        (jnp.logical_not(inner), others, (9, 10, 11, 12, 13, 13, 13, 13, 13, 14, 15, 16, 17, 18, 19, 20, 20, 20, 20, 21, 22, 23, 25)))
    pass_plan = (0, 0, 0, 0, 0, 0, 0, 0, 0, 0, 0, 0, 0, 1, 2, 3, 4, 5, 6, 7, 8, 8, 8)

    def point(p):
        for mask, where, plan in plans:
            group = items[plan[p - 1] if p else 0:plan[p]]
            if group:
                @pl.when(mask)
                def _():
                    for item in group:
                        item(where)
        for r in range(pass_plan[p - 1] if p else 0, pass_plan[p]):
            pass_gate_up(1, r)

    gather_own(0)
    point(0)
    gather_near(0)
    for r in range(8):
        pass_gate_up(0, r)
        point(r + 1)
        if r == 6:
            mix_near()
        if r == 0:
            gather_far(0)
        if r == 3:
            gather_end(0)
    if 6 == 8:
        mix_near()
    point(9)
    pass_down(0, 0)
    wait_own(0)
    load_out.wait()
    for r in range(8):
        take_gate_up(0, r)
    hidden_of(0)
    point(10)
    mix_far()
    reduced(0, tuple((k, functools.partial(point, 11 + k)) for k in range(8)))

    squares = jnp.sum(resid[0] * resid[0], axis=-1, keepdims=True)
    for q in range(1, n_q):
        squares = squares + jnp.sum(resid[q] * resid[q], axis=-1, keepdims=True)
    scale = lax.rsqrt(squares * (1.0 / width) + EPS)
    for q in range(n_q):
        for j in range(n_fs):
            cols = slice(j * dc + q * qc, j * dc + (q + 1) * qc)
            xs[1, u, f, :, cols] = (resid[q, :, j * qc:(j + 1) * qc] * scale * gain2[:, cols]).astype(BF16)

    gather_own(1)
    point(19)
    gather_near(1)
    point(20)
    gather_far(1)
    point(21)
    drain_gate_up(0)
    drain_mix()
    gather_end(1)
    point(22)
    drain_down(0)
    drain_steps(0)
    pass_down(1, 0)
    wait_own(1)
    for r in range(8):
        take_gate_up(1, r)
    hidden_of(1)
    reduced(1, ((2, functools.partial(drain_gate_up, 1)), (4, functools.partial(drain_down, 1))))
    drain_steps(1)

    pltpu.make_async_copy(joined, joined, write_sem).wait()


def gathered_call(mesh, args):
    n_fs, n_tp = mesh.shape["fs"], mesh.shape["tp"]
    tokens, mix_heads, _, gate_first = args[:4]
    rows_in, width = tokens.shape
    dc, hidden = gate_first.shape
    heads = mix_heads.shape[1]
    lane, n_q = 128, n_fs
    n_lane = hidden // lane
    counts = sorted({-(-(j + 1) * n_lane // n_fs) - -(-j * n_lane // n_fs) for j in range(n_fs)})
    most = counts[-1] * lane
    sub, total, qc = rows_in // n_tp, rows_in * n_fs, dc // n_q
    n_x, wide = n_tp // 2, n_fs * qc
    dma = pltpu.SemaphoreType.DMA
    vmem = pl.BlockSpec(memory_space=pltpu.VMEM)
    hbm = pl.BlockSpec(memory_space=pl.ANY)
    lq = (2, n_q)
    return pl.pallas_call(
        functools.partial(gathered, counts, n_fs, n_tp, n_q, lane),
        out_shape=jax.ShapeDtypeStruct((rows_in, width), BF16),
        in_specs=[hbm, hbm, vmem, hbm, hbm, hbm, hbm, vmem, hbm, hbm, hbm],
        out_specs=hbm,
        scratch_shapes=[
            pltpu.VMEM((rows_in, width), BF16),
            pltpu.VMEM((2, 2, width, most), BF16),
            pltpu.VMEM((2, n_q, most, wide), BF16),
            pltpu.VMEM((heads, dc), BF16),
            pltpu.VMEM((2, n_tp, n_fs, sub, width), BF16),
            pltpu.VMEM((n_tp, n_fs, sub, heads), BF16),
            pltpu.VMEM((total, most), BF16),
            pltpu.VMEM((total // 2, wide), F32),
            pltpu.VMEM((*lq, n_tp, n_fs, sub, wide), BF16),
            pltpu.VMEM((*lq, n_x, n_fs, sub, wide), BF16),
            pltpu.VMEM((*lq, n_fs, sub, wide), BF16),
            pltpu.VMEM((*lq, n_fs, sub, wide), BF16),
            pltpu.VMEM((*lq, n_fs, sub, wide), F32),
            pltpu.VMEM((*lq, n_fs, sub, wide), BF16),
            pltpu.VMEM((*lq, sub, wide), BF16),
            pltpu.VMEM((n_q, 2, sub, wide), BF16),
            pltpu.VMEM((n_q, 2, sub, wide), BF16),
            pltpu.VMEM((*lq, sub, wide), BF16),
            pltpu.VMEM((n_q, sub, wide), BF16),
            pltpu.VMEM((n_q, sub, wide), F32),
            pltpu.VMEM((n_q, sub, wide), BF16),
            pltpu.VMEM((n_q, rows_in, wide), BF16),
            dma, dma, dma, dma((2, 2)), dma(lq), dma,
            dma((2, n_fs)), dma((2, 2, 4)), dma((2,)), dma((2, 2, 4)),
            dma((2, n_fs)), dma((*lq, n_fs)), dma((2,)), dma(lq),
            dma((2,)), dma((2, n_fs, 2)), dma((2,)),
            dma((2,)), dma((2, n_fs, 2)), dma((2,)), dma((2,)), dma((2,)), dma((2,)),
            dma((2,)), dma((n_fs,)), dma((2,)),
            *[dma((2,)), dma(lq)] * 3, dma, dma((n_q,)), dma((2,)), dma(lq), dma, dma((n_q,)),
            dma, dma((n_q,)),
        ],
        compiler_params=pltpu.CompilerParams(
            collective_id=0, has_side_effects=True, vmem_limit_bytes=60 * 1024 * 1024),
    )(*args)


def fits(mesh, args):
    tokens, gate = args[0], args[3]
    n_tp = mesh.shape["tp"]
    return (mesh.shape["grp"] == 2 and mesh.shape["fs"] == 4 and n_tp == 4 and tokens.shape[0] % (32 * n_tp) == 0
            and gate.shape[0] % (128 * 4) == 0 and gate.shape[1] % 128 == 0)


def solution(mesh):
    n_fs, n_tp = mesh.shape["fs"], mesh.shape["tp"]

    def local(tokens, mix_heads, norm_first, gate_first, up_first, down_first, out_weight,
              norm_second, gate_second, up_second, down_second):
        args = (tokens, mix_heads, norm_first.reshape(1, -1), gate_first, up_first, down_first, out_weight,
                norm_second.reshape(1, -1), gate_second, up_second, down_second)
        if fits(mesh, args):
            return gathered_call(mesh, args)
        rows_in, width = tokens.shape
        total = rows_in * n_fs
        share = total // n_tp
        dc, hidden = gate_first.shape
        heads = mix_heads.shape[1]
        chunk = rows_in // 2
        n_chunks = total // 2 // chunk
        dma = pltpu.SemaphoreType.DMA
        vmem = pl.BlockSpec(memory_space=pltpu.VMEM)
        hbm = pl.BlockSpec(memory_space=pl.ANY)
        return pl.pallas_call(
            functools.partial(kernel, n_fs, n_tp, chunk),
            out_shape=jax.ShapeDtypeStruct((rows_in, width), BF16),
            in_specs=[vmem, vmem, vmem, hbm, hbm, hbm, hbm, vmem, hbm, hbm, hbm],
            out_specs=vmem,
            scratch_shapes=[
                pltpu.VMEM(gate_first.shape, BF16),
                pltpu.VMEM(up_first.shape, BF16),
                pltpu.VMEM(down_first.shape, BF16),
                pltpu.VMEM(out_weight.shape, BF16),
                pltpu.VMEM(gate_second.shape, BF16),
                pltpu.VMEM(up_second.shape, BF16),
                pltpu.VMEM(down_second.shape, BF16),
                pltpu.VMEM((total, dc), BF16),
                pltpu.VMEM((total, dc), BF16),
                pltpu.VMEM((total, heads), BF16),
                pltpu.VMEM((2, total, hidden), F32),
                pltpu.VMEM((2, total, hidden), BF16),
                pltpu.VMEM((2, total, hidden), BF16),
                pltpu.VMEM((2, total, hidden), BF16),
                pltpu.VMEM((total, hidden), BF16),
                pltpu.VMEM((total, hidden), BF16),
                pltpu.VMEM((total, dc), BF16),
                pltpu.VMEM((n_tp, share, dc), BF16),
                pltpu.VMEM((n_tp, share, dc), BF16),
                pltpu.VMEM((share, dc), F32),
                pltpu.VMEM((n_fs, 8, rows_in), F32),
                pltpu.VMEM((n_fs, 8, share), F32),
                pltpu.VMEM((share, dc), BF16),
                pltpu.VMEM((rows_in, width), BF16),
                dma((7,)), dma((n_fs,)), dma((n_fs,)), dma((n_fs,)), dma((n_fs,)), dma((n_fs,)), dma((n_fs,)),
                dma((n_fs, 2)), dma((n_fs,)),
                dma((2, 2, n_chunks)), dma((2, 2, n_chunks)), dma((2, 2, n_chunks)), dma((2, 2, n_chunks)),
                dma((2, n_tp)), dma((2, n_tp)),
                dma((n_fs,)), dma((n_fs,)), dma((n_tp,)), dma((n_tp,)), dma((n_tp,)), dma((n_tp,)),
                dma((n_tp,)), dma((n_fs,)), dma((n_fs,)), dma((n_fs,)),
            ],
            compiler_params=pltpu.CompilerParams(
                collective_id=0, has_side_effects=True, vmem_limit_bytes=60 * 1024 * 1024),
        )(*args)

    in_specs = (
        P(("grp", "fs"), None),
        P(("grp", "fs"), "tp"),
        P(),
        P("fs", "tp"),
        P("fs", "tp"),
        P("tp", "fs"),
        P("tp", "fs"),
        P(),
        P("fs", "tp"),
        P("fs", "tp"),
        P("tp", "fs"),
    )
    return jax.shard_map(local, mesh=mesh, in_specs=in_specs, out_specs=P(("grp", "fs"), None), check_vma=False)
```

```python
import functools

import jax
import jax.numpy as jnp
from jax import lax
from jax.experimental import pallas as pl
from jax.experimental.pallas import tpu as pltpu
from jax.sharding import PartitionSpec as P

EPS = 0.1
MESH = pl.DeviceIdType.MESH
BF16 = jnp.bfloat16
F32 = jnp.float32


def loop(count, body):
    def step(i, carry):
        body(i)
        return carry

    lax.fori_loop(0, count, step, 0)


def kernel(n_fs, n_tp, chunk,
           tok, mix, gain1, wg1, wu1, wd1, wo, gain2, wg2, wu2, wd2,
           out,
           vg1, vu1, vd1, vo, vg2, vu2, vd2,
           raw, nb2, mixed, grads, sums, in1, in2, hid1, hid2,
           terms, got1, got2, resid, squares1, squares, done_rows, joined,
           wsem, p0_send, p0_recv, fw_send, fw_recv, s1_send, s1_recv, mix_send, mix_recv,
           rs_send, rs_recv, ag_send, ag_recv, tp_send, tp_recv,
           sq_send, sq_recv, nrm_send, nrm_recv, nfw_send, nfw_recv,
           out_send, out_recv, ofw_send, ofw_recv):
    f, t = lax.axis_index("fs"), lax.axis_index("tp")
    rows_in, width = tok.shape
    total = rows_in * n_fs
    share = total // n_tp
    half = total // 2
    n_chunks = half // chunk
    dc = width // n_fs

    weights = ((wg1, vg1), (wu1, vu1), (wd1, vd1), (wo, vo), (wg2, vg2), (wu2, vu2), (wd2, vd2))
    loads = [pltpu.make_async_copy(a, b, wsem.at[i]) for i, (a, b) in enumerate(weights)]
    for load in loads:
        load.start()

    barrier = pltpu.get_barrier_semaphore()

    def greet(i):
        pf, pt = i // n_tp, i % n_tp

        @pl.when(jnp.logical_or(pf != f, pt != t))
        def _():
            pl.semaphore_signal(barrier, inc=1, device_id={"fs": pf, "tp": pt}, device_id_type=MESH)

    loop(n_fs * n_tp, greet)

    def cols(j):
        return pl.ds(pl.multiple_of(j * dc, dc), dc)

    def block(j, size):
        return pl.ds(pl.multiple_of(j * size, size), size)

    def remote(src, dst, send, recv, **where):
        return pltpu.make_async_remote_copy(
            src_ref=src, dst_ref=dst, send_sem=send, recv_sem=recv,
            device_id=where, device_id_type=MESH)

    c_own = t % 2
    partner = t + 1 - 2 * c_own
    half_in = rows_in // 2
    n_pairs = n_tp // 2

    def squares_of(x):
        own = jnp.sum(x * x, axis=-1, keepdims=True)
        return jnp.transpose(jnp.broadcast_to(own, (x.shape[0], 128)))[0:8, :]

    def scale_of(summed):
        column = jnp.transpose(jnp.broadcast_to(summed[0:1, :], (128, summed.shape[1])))[:, 0:1]
        return lax.rsqrt(column * (1.0 / width) + EPS)

    def piece_of(slot):
        return pl.ds(pl.multiple_of(slot * rows_in + c_own * half_in, half_in), half_in)

    def p0_copy(j, slot):
        return remote(tok.at[block(c_own, half_in), cols(j)], raw.at[piece_of(slot), :],
                      p0_send.at[j], p0_recv.at[slot], fs=j)

    def fw_copy(slot):
        place = raw.at[piece_of(slot), :]
        return remote(place, place, fw_send.at[slot], fw_recv.at[slot], tp=partner)

    def s1_copy(j, slot):
        return remote(squares1.at[f], squares1.at[slot], s1_send.at[j], s1_recv.at[slot], fs=j)

    def sq_copy(j, slot):
        return remote(squares.at[f], squares.at[slot], sq_send.at[j], sq_recv.at[slot], fs=j)

    def mix_copy(slot, side, where):
        place = mixed.at[block(slot, rows_in), :]
        return remote(place, place, mix_send.at[slot, side], mix_recv.at[slot], fs=where)

    mixed[block(f, rows_in), :] = mix[...]
    pl.semaphore_wait(barrier, n_fs * n_tp - 1)

    def p0_start(i):
        p0_copy((f + 1 + i) % n_fs, f).start()

    loop(n_fs - 1, p0_start)
    squares1[f] = squares_of(tok[...].astype(F32))

    def s1_start(i):
        s1_copy((f + 1 + i) % n_fs, f).start()

    loop(n_fs - 1, s1_start)

    @pl.when(f < n_fs - 1)
    def _():
        mix_copy(f, 0, f + 1).start()

    @pl.when(f > 0)
    def _():
        mix_copy(f, 1, f - 1).start()

    raw[block(f, rows_in), :] = tok[:, cols(f)]

    def gates_one(j):
        rows = block(j, rows_in)
        x = (raw[rows, :].astype(F32) * scale_of(squares1[j]) * gain1[:, cols(f)]).astype(BF16)
        grads[0, rows, :] = jnp.dot(x, vg1[...], preferred_element_type=F32)
        grads[1, rows, :] = jnp.dot(x, vu1[...], preferred_element_type=F32)

    def side_of(side):
        hops = jnp.where(side == 0, n_fs - 1 - f, f)
        toward = jnp.where(side == 0, f - 1, f + 1)
        away = jnp.where(side == 0, f + 1, f - 1)
        return hops, toward, away

    near = jnp.where(2 * f >= n_fs, 0, 1)

    def chain(layer, arrived, hid, with_mix):
        def rows_of(side, c):
            return pl.ds(pl.multiple_of(side * half + c * chunk, chunk), chunk)

        def rs_copy(side, c, where):
            rows = rows_of(side, c)
            return remote(sums.at[:, rows, :], arrived.at[:, rows, :],
                          rs_send.at[layer, side, c], rs_recv.at[layer, side, c], fs=where)

        def ag_copy(side, c, where):
            rows = rows_of(side, c)
            return remote(hid.at[rows, :], hid.at[rows, :],
                          ag_send.at[layer, side, c], ag_recv.at[layer, side, c], fs=where)

        for side in (0, 1):
            hops, toward, away = side_of(side)

            @pl.when(hops == 0)
            def _():
                def first(c):
                    rows = rows_of(side, c)
                    sums[:, rows, :] = grads[:, rows, :].astype(BF16)
                    rs_copy(side, c, toward).start()

                loop(n_chunks, first)

        def step(s):
            for k in (0, 1):
                side = near if k == 0 else 1 - near
                hops, toward, away = side_of(side)
                c = s - hops

                @pl.when(jnp.logical_and(hops > 0, jnp.logical_and(c >= 0, c < n_chunks)))
                def _():
                    rows = rows_of(side, c)
                    rs_copy(side, c, f).wait_recv()

                    @pl.when(hops < n_fs - 1)
                    def _():
                        sums[:, rows, :] = (grads[:, rows, :] + arrived[:, rows, :].astype(F32)).astype(BF16)
                        rs_copy(side, c, toward).start()

                    @pl.when(hops == n_fs - 1)
                    def _():
                        g = grads[0, rows, :] + arrived[0, rows, :].astype(F32)
                        v = grads[1, rows, :] + arrived[1, rows, :].astype(F32)
                        hid[rows, :] = (g / (1.0 + jnp.exp(-g)) * v).astype(BF16)
                        ag_copy(side, c, away).start()

            if with_mix:
                @pl.when(jnp.logical_and(s > 0, s < n_fs))
                def _():
                    low, high = f - s, f + s

                    @pl.when(low >= 0)
                    def _():
                        mix_copy(low, 0, f).wait_recv()

                        @pl.when(f < n_fs - 1)
                        def _():
                            mix_copy(low, 0, f + 1).start()

                    @pl.when(high < n_fs)
                    def _():
                        mix_copy(high, 1, f).wait_recv()

                        @pl.when(f > 0)
                        def _():
                            mix_copy(high, 1, f - 1).start()

        loop(n_chunks + n_fs - 1, step)

        def relay(c):
            for k in (0, 1):
                side = 1 - near if k == 0 else near
                hops, toward, away = side_of(side)

                @pl.when(hops < n_fs - 1)
                def _():
                    ag_copy(side, c, f).wait_recv()

                    @pl.when(hops > 0)
                    def _():
                        ag_copy(side, c, away).start()

        def drain(c):
            for side in (0, 1):
                hops, toward, away = side_of(side)

                @pl.when(hops < n_fs - 1)
                def _():
                    rs_copy(side, c, f).wait_send()

                @pl.when(hops > 0)
                def _():
                    ag_copy(side, c, f).wait_send()

        return relay, lambda: loop(n_chunks, drain)

    def tp_copy(layer, j, slot, got):
        return remote(terms.at[block(j, share), :], got.at[slot],
                      tp_send.at[layer, j], tp_recv.at[layer, slot], tp=j)

    def down(layer, relay, hid, vd, got, with_mix):
        per_block = n_chunks // n_pairs

        def piece(b):
            def inner(i):
                relay(b * per_block + i)

            loop(per_block, inner)
            for side in (0, 1):
                j = side * n_pairs + b
                rows = block(j, share)
                value = 0.5 * jnp.dot(hid[rows, :], vd[...], preferred_element_type=F32)
                if with_mix:
                    value = value + jnp.dot(mixed[rows, :], vo[...], preferred_element_type=F32)
                terms[rows, :] = value.astype(BF16)

                @pl.when(j != t)
                def _():
                    tp_copy(layer, j, t, got).start()

        loop(n_pairs, piece)

    def reduce_tp(layer, got, start_value):
        resid[...] = start_value + terms[block(t, share), :].astype(F32)

        def add(i):
            j = (t + 1 + i) % n_tp
            tp_copy(layer, j, j, got).wait_recv()
            resid[...] = resid[...] + got[j].astype(F32)

        loop(n_tp - 1, add)

        def drain(i):
            j = (t + 1 + i) % n_tp
            tp_copy(layer, j, t, got).wait_send()

        loop(n_tp - 1, drain)

    loads[0].wait()
    loads[1].wait()
    gates_one(f)

    def pass_on(i):
        j = (f + 1 + i) % n_fs
        p0_copy(j, j).wait_recv()
        fw_copy(j).start()

    loop(n_fs - 1, pass_on)

    def other_rows(i):
        j = (f + 1 + i) % n_fs
        s1_copy(j, j).wait_recv()
        fw_in(j).wait_recv()
        gates_one(j)

    def fw_in(slot):
        start = pl.multiple_of(slot * rows_in + (1 - c_own) * half_in, half_in)
        place = raw.at[pl.ds(start, half_in), :]
        return remote(place, place, fw_send.at[slot], fw_recv.at[slot], tp=partner)

    loop(n_fs - 1, other_rows)
    relay_one, drain_one = chain(0, in1, hid1, True)
    loads[2].wait()
    loads[3].wait()
    down(0, relay_one, hid1, vd1, got1, True)
    reduce_tp(0, got1, raw[block(t, share), :].astype(F32))

    squares[f] = squares_of(resid[...])

    def sq_start(i):
        sq_copy((f + 1 + i) % n_fs, f).start()

    def sq_wait(i):
        j = (f + 1 + i) % n_fs
        sq_copy(j, j).wait_recv()

    loop(n_fs - 1, sq_start)
    drain_one()
    loop(n_fs - 1, sq_wait)
    summed = squares[0]
    for j in range(1, n_fs):
        summed = summed + squares[j]
    nb2[block(t, share), :] = (resid[...] * scale_of(summed) * gain2[:, cols(f)]).astype(BF16)

    def nrm_copy(j, slot):
        place = nb2.at[block(slot, share), :]
        return remote(place, place, nrm_send.at[j], nrm_recv.at[slot], tp=j)

    def nfw_copy(slot):
        place = nb2.at[block(slot, share), :]
        return remote(place, place, nfw_send.at[slot], nfw_recv.at[slot], tp=partner)

    def same_core(i):
        return (t + 2 + 2 * i) % n_tp

    def nrm_start(i):
        nrm_copy(same_core(i), t).start()

    loop(n_pairs - 1, nrm_start)
    nfw_copy(t).start()
    loads[4].wait()
    loads[5].wait()

    def gates_two(j):
        rows = block(j, share)
        x = nb2[rows, :]
        grads[0, rows, :] = jnp.dot(x, vg2[...], preferred_element_type=F32)
        grads[1, rows, :] = jnp.dot(x, vu2[...], preferred_element_type=F32)

    gates_two(t)
    nfw_copy(partner).wait_recv()
    gates_two(partner)

    def nrm_pass(i):
        j = same_core(i)
        nrm_copy(j, j).wait_recv()
        nfw_copy(j).start()
        gates_two(j)

    loop(n_pairs - 1, nrm_pass)

    def nrm_last(i):
        j = (partner + 2 + 2 * i) % n_tp
        nfw_copy(j).wait_recv()
        gates_two(j)

    loop(n_pairs - 1, nrm_last)
    relay_two, drain_two = chain(1, in2, hid2, False)
    loads[6].wait()
    down(1, relay_two, hid2, vd2, got2, False)
    reduce_tp(1, got2, resid[...])
    done_rows[...] = resid[...].astype(BF16)

    def out_copy(j, slot):
        return remote(done_rows, joined.at[:, cols(slot)], out_send.at[j], out_recv.at[slot], fs=t, tp=j)

    def ofw_copy(slot):
        place = joined.at[:, cols(slot)]
        return remote(place, place, ofw_send.at[slot], ofw_recv.at[slot], tp=partner)

    def out_start(i):
        j = c_own + 2 * i

        @pl.when(jnp.logical_or(f != t, j != t))
        def _():
            out_copy(j, f).start()

    loop(n_pairs, out_start)

    @pl.when(f == t)
    def _():
        joined[:, cols(f)] = done_rows[...]

    takes = c_own == f % 2

    @pl.when(takes)
    def _():
        def take(i):
            j = (f + i) % n_fs

            @pl.when(jnp.logical_or(f != t, j != f))
            def _():
                out_copy(t, j).wait_recv()

            ofw_copy(j).start()

        loop(n_fs, take)

    @pl.when(jnp.logical_not(takes))
    def _():
        def take(i):
            ofw_copy((f + i) % n_fs).wait_recv()

        loop(n_fs, take)

    out[...] = joined[...]

    drain_two()

    def last_fs(i):
        j = (f + 1 + i) % n_fs
        p0_copy(j, f).wait_send()
        fw_copy(j).wait_send()
        s1_copy(j, f).wait_send()
        sq_copy(j, f).wait_send()

    loop(n_fs - 1, last_fs)

    def last_mix(j):
        @pl.when(jnp.logical_and(j <= f, f < n_fs - 1))
        def _():
            mix_copy(j, 0, f).wait_send()

        @pl.when(jnp.logical_and(j >= f, f > 0))
        def _():
            mix_copy(j, 1, f).wait_send()

        @pl.when(takes)
        def _():
            ofw_copy(j).wait_send()

    loop(n_fs, last_mix)

    def last_nrm(i):
        nrm_copy(same_core(i), t).wait_send()

    loop(n_pairs - 1, last_nrm)

    def last_out(i):
        j = c_own + 2 * i
        nfw_copy(j).wait_send()

        @pl.when(jnp.logical_or(f != t, j != t))
        def _():
            out_copy(j, f).wait_send()

    loop(n_pairs, last_out)


def by_count(counts, value, body):
    for n in counts:
        if len(counts) == 1:
            body(n)
        else:
            pl.when(value == n)(functools.partial(body, n))


def gathered(counts, n_fs, n_tp, n_q, lane,
             tok, mix, gain1, wg1, wu1, wd1, wo, gain2, wg2, wu2, wd2,
             out,
             rows_of_me, wgu, wdb, wob, xs, mixed, hid, acc, part, r1, s1, r2, full, zs, rp, rr, zf, rf, rg, resid, done, joined,
             tok_sem, mix_sem, write_sem, wl_sem, dl_sem, wo_sem,
             wz_send, wz_recv, wy_send, wy_recv, dz_send, dz_recv, dy_send, dy_recv,
             ag_send, ag_recv, agr_send, ax_send, ax_recv, ad_send, ad_recv, af_send, af_recv,
             mz_send, mz_recv, mr_send,
             r1_send, r1_recv, r2_send, r2_recv, rp_send, rp_recv, rr_send, rr_recv, rf_send, rf_recv, rg_send, rg_recv,
             o_send, o_recv):
    g, f, t = lax.axis_index("grp"), lax.axis_index("fs"), lax.axis_index("tp")
    rows_in, width = tok.shape
    dc, hidden = wg1.shape
    n_x = n_tp // 2
    core, x = t % 2, t // 2
    sub = rows_in // n_tp
    unit = n_fs * sub
    u = core * n_x + x
    u_x = core * n_x + 1 - x
    u_pair = (1 - core) * n_x + x
    u_diag = (1 - core) * n_x + 1 - x
    t_x = (t + 2) % n_tp
    t_pair = t + 1 - 2 * core
    t_diag = (t_pair + 2) % n_tp
    pair = f + 1 - 2 * (f % 2)
    far0 = jnp.where(f < 2, 2, 0)
    inner = jnp.logical_or(f == 1, f == 2)
    bridge = jnp.where(f < 2, 2, 1)
    others = (jnp.where(f < 2, n_fs - 1, 0), bridge, pair)
    n_k = 4
    piece = dc // (2 * n_k)
    qc = dc // n_q
    n_lane = hidden // lane
    most = max(counts)
    gate_up = ((wg1, wu1), (wg2, wu2))
    downs = (wd1, wd2)

    def first(j):
        return (j * n_lane + (1 - core) * (n_fs - 1)) // n_fs

    def count(j):
        return first(j + 1) - first(j)

    mine = count(f)

    def at(i, size):
        return pl.ds(pl.multiple_of(i * size, size), size)

    def remote(src, dst, send, recv, **where):
        return pltpu.make_async_remote_copy(
            src_ref=src, dst_ref=dst, send_sem=send, recv_sem=recv,
            device_id=where, device_id_type=MESH)

    def load_gate_up(n, l, m):
        cols = pl.ds(pl.multiple_of(first(f) * lane, lane), n * lane)
        return pltpu.make_async_copy(
            gate_up[l][m].at[:, cols], wgu.at[l, m, at(f, dc), pl.ds(0, n * lane)], wl_sem.at[l, m])

    def load_down(n, l, q):
        rows = pl.ds(pl.multiple_of(first(f) * lane, lane), n * lane)
        return pltpu.make_async_copy(
            downs[l].at[rows, at(q, qc)], wdb.at[l, q, pl.ds(0, n * lane), at(f, qc)], dl_sem.at[l, q])

    def start_loads(n):
        for l in (0, 1):
            for m in (0, 1):
                load_gate_up(n, l, m).start()
            for q in range(n_q):
                load_down(n, l, q).start()
        if n < most:
            rest = pl.ds(n * lane, (most - n) * lane)
            wgu[:, :, :, rest] = jnp.zeros((2, 2, width, (most - n) * lane), BF16)
            wdb[:, :, rest, :] = jnp.zeros((2, n_q, (most - n) * lane, n_fs * qc), BF16)

    barrier = pltpu.get_barrier_semaphore()
    for i in range(n_fs - 1):
        pl.semaphore_signal(barrier, inc=1, device_id={"fs": others[i]}, device_id_type=MESH)
    pl.semaphore_signal(barrier, inc=1, device_id={"grp": 1 - g}, device_id_type=MESH)
    for j in (t_x, t_pair, t_diag):
        pl.semaphore_signal(barrier, inc=1, device_id={"tp": j}, device_id_type=MESH)

    load_tok = pltpu.make_async_copy(tok, rows_of_me, tok_sem)
    load_tok.start()
    load_mix = [pltpu.make_async_copy(
        mix.at[j * sub:(j + 1) * sub, :], mixed.at[(j % 2) * n_x + j // 2, f], mix_sem) for j in range(n_tp)]
    for load in load_mix:
        load.start()
    by_count(counts, mine, start_loads)
    load_out = pltpu.make_async_copy(wo, wob, wo_sem)
    load_out.start()

    def normed(values, gain):
        squares = jnp.sum(values * values, axis=-1, keepdims=True)
        return values * lax.rsqrt(squares * (1.0 / width) + EPS) * gain

    load_tok.wait()
    own = rows_of_me[at(t, sub), :].astype(F32)
    xs[0, u, f] = normed(own, gain1[...]).astype(BF16)
    for j in range(n_tp):
        @pl.when(j != t)
        def _():
            rows = rows_of_me[j * sub:(j + 1) * sub, :].astype(F32)
            xs[0, (j % 2) * n_x + j // 2, f] = normed(rows, gain1[...]).astype(BF16)
    for q in range(n_q):
        for j in range(n_fs):
            resid[q, :, j * qc:(j + 1) * qc] = own[:, j * dc + q * qc:j * dc + (q + 1) * qc]
    pltpu.make_async_copy(mixed.at[:, f], mixed.at[:, f], mix_sem).wait()
    pl.semaphore_wait(barrier, n_fs - 1 + 1 + n_tp - 1)

    def send_one(n, l, m, k, j):
        cols = pl.ds(pl.multiple_of(first(j) * lane, lane), n * lane)
        remote(gate_up[l][m].at[at(n_k * g + k, piece), cols],
               wgu.at[l, m, at(n_k * (2 * f + g) + k, piece), pl.ds(0, n * lane)],
               wz_send.at[l, j], wz_recv.at[l, m, k], fs=j).start()

    def send_gate_up(l, r, where=others):
        for j in where:
            by_count(counts, count(j), lambda n, j=j: send_one(n, l, r % 2, r // 2, j))

    def gate_up_y(n, l, m, k, j):
        place = wgu.at[l, m, at(n_k * (2 * j + g) + k, piece), pl.ds(0, n * lane)]
        return remote(place, place, wy_send.at[l], wy_recv.at[l, m, k], grp=1 - g)

    def all_pieces(n, l, m, k, send, recv):
        place = wgu.at[l, m, pl.ds(0, len(others) * piece), pl.ds(0, n * lane)]
        return remote(place, place, send, recv, grp=1 - g)

    def pass_gate_up(l, r):
        m, k = r % 2, r // 2

        def go(n):
            all_pieces(n, l, m, k, wz_send.at[l, pair], wz_recv.at[l, m, k]).wait_recv()
            for j in others:
                gate_up_y(n, l, m, k, j).start()

        by_count(counts, mine, go)

    def take_gate_up(l, r):
        m, k = r % 2, r // 2
        by_count(counts, mine, lambda n: all_pieces(n, l, m, k, wy_send.at[l], wy_recv.at[l, m, k]).wait_recv())

    def down_part(n, l, q, j, side):
        size = n * lane // 2
        return wdb.at[l, q, at(side, size), at(j, qc)]

    def send_down(l, q, where=others):
        for j in where:
            def go(n, j=j):
                size = n * lane // 2
                rows = pl.ds(pl.multiple_of(first(j) * lane + g * size, lane // 2), size)
                remote(downs[l].at[rows, at(q, qc)], down_part(n, l, q, f, g),
                       dz_send.at[l, j], dz_recv.at[l, q, f], fs=j).start()

            by_count(counts, count(j), go)

    def down_y(n, l, q, j):
        place = down_part(n, l, q, j, g)
        return remote(place, place, dy_send.at[l], dy_recv.at[l, q], grp=1 - g)

    def all_downs(n, l, q, send, recv):
        place = wdb.at[l, q, pl.ds(0, n * lane // 2), pl.ds(0, len(others) * qc)]
        return remote(place, place, send, recv, grp=1 - g)

    def z_block(l, j, h, send, where):
        place = xs.at[l, u, j, at(h, sub // 2)]
        return remote(place, place, send, ag_recv.at[l, j, h], fs=where)

    def x_block(l, j, who, h):
        place = xs.at[l, who, j, at(h, sub // 2)]
        return remote(place, place, ax_send.at[l], ax_recv.at[l, j, h], tp=t_x)

    def pair_block(l, j, who, h):
        place = xs.at[l, who, j, at(h, sub // 2)]
        return remote(place, place, ad_send.at[l], ad_recv.at[l], tp=t_pair)

    def diag_block(l, j, who, h):
        place = xs.at[l, who, j, at(h, sub // 2)]
        return remote(place, place, af_send.at[l], af_recv.at[l], tp=t_pair)

    def pass_rows(l, j, h):
        x_block(l, j, u, h).start()
        pair_block(l, j, u, h).start()

    def gather_own(l):
        for h in (0, 1):
            z_block(l, f, h, ag_send.at[l], bridge).start()
        for h in (0, 1):
            z_block(l, f, h, ag_send.at[l], pair).start()
            if l == 1:
                pass_rows(l, f, h)

    def gather_near(l):
        for h in (0, 1):
            for k in (0, 1):
                @pl.when(inner)
                def _():
                    j = far0 + k
                    z_block(l, j, h, agr_send.at[l], j).wait_recv()
                    z_block(l, j, h, agr_send.at[l], pair).start()
                    pass_rows(l, j, h)

        for h in (0, 1):
            z_block(l, pair, h, ag_send.at[l], pair).wait_recv()
            pass_rows(l, pair, h)

    def gather_far(l):
        for h in (0, 1):
            for k in (0, 1):
                @pl.when(jnp.logical_not(inner))
                def _():
                    j = far0 + k
                    z_block(l, j, h, agr_send.at[l], j).wait_recv()
                    pass_rows(l, j, h)

    def gather_end(l):
        blocks = [(j, h) for j in (far0, far0 + 1, pair) for h in (0, 1)]
        if l == 1:
            blocks = [(f, 0), (f, 1)] + blocks
        for j, h in blocks:
            x_block(l, j, u_x, h).wait_recv()
            diag_block(l, j, u_x, h).start()
        rows = xs.at[l, 0, pl.ds(0, len(blocks) // 2)]
        remote(rows, rows, ad_send.at[l], ad_recv.at[l], tp=t_pair).wait_recv()
        remote(rows, rows, af_send.at[l], af_recv.at[l], tp=t_pair).wait_recv()

    def mix_block(j, send, where):
        place = mixed.at[:, j]
        return remote(place, place, send, mz_recv.at[j], fs=where)

    def mix_near():
        @pl.when(inner)
        def _():
            for k in (0, 1):
                j = far0 + k
                mix_block(j, mr_send.at[k], j).wait_recv()
                mix_block(j, mr_send.at[k], pair).start()

    def mix_far():
        @pl.when(jnp.logical_not(inner))
        def _():
            for k in (0, 1):
                mix_block(far0 + k, mr_send.at[k], far0 + k).wait_recv()

        mix_block(pair, mz_send.at[1], pair).wait_recv()

    def hidden_of(l):
        def step(i):
            rows = xs[l, at(i, n_x)].reshape(n_x * unit, width)
            gate = jnp.dot(rows, wgu[l, 0], preferred_element_type=F32)
            value = jnp.dot(rows, wgu[l, 1], preferred_element_type=F32)
            hid[at(i, n_x * unit), :] = (gate / (1.0 + jnp.exp(-gate)) * value).astype(BF16)

        loop(2, step)

    def s1_copy(l, q):
        return remote(part.at[l, q, at(1 - core, n_x)], r1.at[l, q], r1_send.at[l], r1_recv.at[l, q], tp=t_pair)

    def s2_copy(l, q):
        return remote(s1.at[l, q], r2.at[l, q], r2_send.at[l], r2_recv.at[l, q], tp=t_x)

    def pair_copy(l, q):
        return remote(zs.at[l, q, pair], rp.at[l, q], rp_send.at[l], rp_recv.at[l, q], fs=pair)

    def relay_copy(q):
        return remote(zs.at[0, q, pl.ds(far0, 2)], rr.at[q], rr_send, rr_recv.at[q], fs=pair)

    def far_copy(q, k, where):
        return remote(zf.at[q, k], rf.at[0, q], rf_send.at[0], rf_recv.at[0, q], fs=where)

    def straight(q, k, where):
        return remote(zs.at[1, q, far0 + k], rg.at[q], rg_send, rg_recv.at[q], fs=where)

    def straight_inner(q, k, where):
        return remote(zs.at[1, q, far0 + k], rf.at[1, q], rf_send.at[1], rf_recv.at[1, q], fs=where)

    def out_copy(q, where, who):
        return remote(done.at[q], joined.at[q, at(who, sub)], o_send, o_recv.at[q], tp=where)

    def pass_down(l, q):
        def go(n):
            for j in others:
                place = down_part(n, l, q, j, g)
                remote(place, place, dz_send.at[l, j], dz_recv.at[l, q, j], fs=j).wait_recv()
                down_y(n, l, q, j).start()

        by_count(counts, mine, go)

    def write_copy(q, j):
        return pltpu.make_async_copy(
            joined.at[q, :, at(j, qc)], out.at[:, pl.ds(pl.multiple_of(j * dc + q * qc, qc), qc)], write_sem)

    def reduced(l, hooks):
        def multiply(q):
            @pl.when(q < n_q - 1)
            def _():
                pass_down(l, q + 1)

            def ready(n):
                all_downs(n, l, q, dy_send.at[l], dy_recv.at[l, q]).wait_recv()
                load_down(n, l, q).wait()

            by_count(counts, mine, ready)

            def side(i):
                c = (1 - core) * (1 - i) + core * i
                value = 0.5 * jnp.dot(hid[at(c, n_x * unit), :], wdb[l, q], preferred_element_type=F32)
                if l == 0:
                    acc[...] = value
                    heads = mixed[at(c, n_x)].reshape(n_x * unit, mixed.shape[-1])
                    acc[:, at(f, qc)] = acc[:, at(f, qc)] + jnp.dot(
                        heads, wob[:, at(q, qc)], preferred_element_type=F32)
                    value = acc[...]
                part[l, q, at(c, n_x)] = value.astype(BF16).reshape(n_x, n_fs, sub, n_fs * qc)

                @pl.when(i == 0)
                def _():
                    s1_copy(l, q).start()

            loop(2, side)

        def across(q):
            s1_copy(l, q).wait_recv()
            s1[l, q] = (part[l, q, u_x].astype(F32) + r1[l, q, 1 - x].astype(F32)).astype(BF16)
            s2_copy(l, q).start()

        def along(q):
            s2_copy(l, q).wait_recv()
            value = part[l, q, u].astype(F32) + r1[l, q, x].astype(F32) + r2[l, q].astype(F32)
            full[l, q] = value
            zs[l, q] = value.astype(BF16)

            if l == 0:
                pl.when(jnp.logical_not(inner))(lambda: relay_copy(q).start())
            else:
                @pl.when(inner)
                def _():
                    for k in (0, 1):
                        straight_inner(q, k, far0 + k).start()

                @pl.when(jnp.logical_not(inner))
                def _():
                    for k in (0, 1):
                        straight(q, k, far0 + k).start()

            pair_copy(l, q).start()

        def relay(q):
            @pl.when(inner)
            def _():
                relay_copy(q).wait_recv()
                for k in (0, 1):
                    zf[q, k] = (full[0, q, far0 + k] + rr[q, k].astype(F32)).astype(BF16)
                    far_copy(q, k, far0 + k).start()

        def finish(q):
            pair_copy(l, q).wait_recv()
            value = full[l, q, f] + rp[l, q].astype(F32)
            if l == 0:
                far_copy(q, 0, far0).wait_recv()
            else:
                straight_inner(q, 0, far0).wait_recv()
                straight(q, 0, far0).wait_recv()
                value = value + rg[q].astype(F32)
            value = resid[q] + (value + rf[l, q].astype(F32))
            if l == 0:
                resid[q] = value
            else:
                done[q] = value.astype(BF16)
                joined[q, at(t, sub)] = value.astype(BF16)
                for where in (t_x, t_diag, t_pair):
                    out_copy(q, where, t).start()

        def write(q):
            rows = joined.at[q, pl.ds(0, (n_tp - 1) * sub)]
            remote(rows, rows, o_send, o_recv.at[q], tp=t_pair).wait_recv()
            for j in range(n_fs):
                write_copy(q, j).start()

        stages = [(multiply, 0), (across, 0), (along, 1)]
        stages += [(relay, 2), (finish, 4)] if l == 0 else [(finish, 2), (write, 3)]

        def step(s):
            for stage, lag in stages:
                @pl.when(jnp.logical_and(s >= lag, s < n_q + lag))
                def _():
                    stage(s - lag)

            for when, hook in hooks:
                pl.when(s == when)(hook)

        loop(n_q + stages[-1][1], step)

    def sent(ref, sem):
        remote(ref, ref, sem, ag_recv.at[0, 0, 0], tp=t_pair).wait_send()

    def drain_gate_up(l):
        for j in others:
            by_count(counts, count(j), lambda n, j=j: sent(
                wgu.at[l, 0, pl.ds(0, dc), pl.ds(0, n * lane)], wz_send.at[l, j]))
        by_count(counts, mine, lambda n: sent(
            wgu.at[l, 0, pl.ds(0, len(others) * dc), pl.ds(0, n * lane)], wy_send.at[l]))
        sent(xs.at[l, 0, pl.ds(0, 2)], ag_send.at[l])
        pl.when(inner)(lambda: sent(xs.at[l, 0, pl.ds(0, 2)], agr_send.at[l]))
        rows = xs.at[l, 0, pl.ds(0, 4 if l == 1 else 3)]
        for sem in (ax_send, ad_send, af_send):
            sent(rows, sem.at[l])

    def drain_mix():
        mix_block(f, mz_send.at[0], bridge).wait_send()
        mix_block(f, mz_send.at[1], pair).wait_send()

        @pl.when(inner)
        def _():
            for k in (0, 1):
                mix_block(far0 + k, mr_send.at[k], pair).wait_send()

    def drain_down(l):
        for j in others:
            by_count(counts, count(j), lambda n, j=j: sent(
                wdb.at[l, 0, pl.ds(0, n * lane // 2)], dz_send.at[l, j]))
        by_count(counts, mine, lambda n: sent(
            wdb.at[l, pl.ds(0, len(others)), pl.ds(0, n * lane // 2)], dy_send.at[l]))

    def drain_steps(l):
        sent(part.at[l, :, pl.ds(0, n_x)], r1_send.at[l])
        sent(s1.at[l], r2_send.at[l])
        sent(zs.at[l, 0], rp_send.at[l])
        pl.when(inner)(lambda: sent(zs.at[l, pl.ds(0, 2)], rf_send.at[l]))
        pl.when(jnp.logical_not(inner))(lambda: sent(zs.at[l, pl.ds(0, 2)], rg_send if l else rr_send))
        if l == 1:
            sent(joined.at[:, pl.ds(0, (n_tp - 1) * sub)], o_send)

    def wait_own(l):
        for m in (0, 1):
            by_count(counts, mine, lambda n, m=m: load_gate_up(n, l, m).wait())

    cross, near = others[:2], others[2:]

    def mix_to(where):
        if where is not near:
            mix_block(f, mz_send.at[0], bridge).start()
        if where is not cross:
            mix_block(f, mz_send.at[1], pair).start()

    items = [
        *(functools.partial(send_gate_up, 0, r) for r in range(8)),
        *(functools.partial(send_down, 0, q) for q in range(n_q)),
        *(functools.partial(send_gate_up, 1, r) for r in range(8)),
        *(functools.partial(send_down, 1, q) for q in range(n_q))]
    items.insert(5, mix_to)
    plans = (
        (inner, cross, (13, 13, 13, 13, 13, 13, 13, 13, 13, 15, 16, 17, 18, 19, 20, 21, 21, 21, 21, 21, 22, 24, 25)),
        (inner, near, (13, 13, 13, 13, 13, 13, 13, 13, 13, 15, 16, 17, 18, 19, 20, 21, 21, 21, 21, 21, 22, 24, 25)),
        (jnp.logical_not(inner), others, (9, 10, 11, 12, 13, 13, 13, 13, 13, 14, 15, 16, 17, 18, 19, 20, 20, 20, 20, 21, 22, 23, 25)))
    pass_plan = (0, 0, 0, 0, 0, 0, 0, 0, 0, 0, 0, 0, 0, 1, 2, 3, 4, 5, 6, 6, 7, 8, 8)

    def point(p):
        for mask, where, plan in plans:
            group = items[plan[p - 1] if p else 0:plan[p]]
            if group:
                @pl.when(mask)
                def _():
                    for item in group:
                        item(where)
        for r in range(pass_plan[p - 1] if p else 0, pass_plan[p]):
            pass_gate_up(1, r)

    gather_own(0)
    point(0)
    gather_near(0)
    for r in range(8):
        pass_gate_up(0, r)
        point(r + 1)
        if r == 6:
            mix_near()
        if r == 0:
            gather_far(0)
        if r == 3:
            gather_end(0)
    if 6 == 8:
        mix_near()
    point(9)
    pass_down(0, 0)
    wait_own(0)
    load_out.wait()
    for r in range(8):
        take_gate_up(0, r)
    hidden_of(0)
    point(10)
    mix_far()
    reduced(0, tuple((k, functools.partial(point, 11 + k)) for k in range(8)))

    squares = jnp.sum(resid[0] * resid[0], axis=-1, keepdims=True)
    for q in range(1, n_q):
        squares = squares + jnp.sum(resid[q] * resid[q], axis=-1, keepdims=True)
    scale = lax.rsqrt(squares * (1.0 / width) + EPS)
    for q in range(n_q):
        for j in range(n_fs):
            cols = slice(j * dc + q * qc, j * dc + (q + 1) * qc)
            xs[1, u, f, :, cols] = (resid[q, :, j * qc:(j + 1) * qc] * scale * gain2[:, cols]).astype(BF16)

    gather_own(1)
    point(19)
    gather_near(1)
    point(20)
    gather_far(1)
    point(21)
    drain_gate_up(0)
    drain_mix()
    gather_end(1)
    point(22)
    drain_down(0)
    drain_steps(0)
    pass_down(1, 0)
    wait_own(1)
    for r in range(8):
        take_gate_up(1, r)
    hidden_of(1)
    reduced(1, ((2, functools.partial(drain_gate_up, 1)), (4, functools.partial(drain_down, 1))))
    drain_steps(1)

    pltpu.make_async_copy(joined, joined, write_sem).wait()


def gathered_call(mesh, args):
    n_fs, n_tp = mesh.shape["fs"], mesh.shape["tp"]
    tokens, mix_heads, _, gate_first = args[:4]
    rows_in, width = tokens.shape
    dc, hidden = gate_first.shape
    heads = mix_heads.shape[1]
    lane, n_q = 128, n_fs
    n_lane = hidden // lane
    counts = sorted({-(-(j + 1) * n_lane // n_fs) - -(-j * n_lane // n_fs) for j in range(n_fs)})
    most = counts[-1] * lane
    sub, total, qc = rows_in // n_tp, rows_in * n_fs, dc // n_q
    n_x, wide = n_tp // 2, n_fs * qc
    dma = pltpu.SemaphoreType.DMA
    vmem = pl.BlockSpec(memory_space=pltpu.VMEM)
    hbm = pl.BlockSpec(memory_space=pl.ANY)
    lq = (2, n_q)
    return pl.pallas_call(
        functools.partial(gathered, counts, n_fs, n_tp, n_q, lane),
        out_shape=jax.ShapeDtypeStruct((rows_in, width), BF16),
        in_specs=[hbm, hbm, vmem, hbm, hbm, hbm, hbm, vmem, hbm, hbm, hbm],
        out_specs=hbm,
        scratch_shapes=[
            pltpu.VMEM((rows_in, width), BF16),
            pltpu.VMEM((2, 2, width, most), BF16),
            pltpu.VMEM((2, n_q, most, wide), BF16),
            pltpu.VMEM((heads, dc), BF16),
            pltpu.VMEM((2, n_tp, n_fs, sub, width), BF16),
            pltpu.VMEM((n_tp, n_fs, sub, heads), BF16),
            pltpu.VMEM((total, most), BF16),
            pltpu.VMEM((total // 2, wide), F32),
            pltpu.VMEM((*lq, n_tp, n_fs, sub, wide), BF16),
            pltpu.VMEM((*lq, n_x, n_fs, sub, wide), BF16),
            pltpu.VMEM((*lq, n_fs, sub, wide), BF16),
            pltpu.VMEM((*lq, n_fs, sub, wide), BF16),
            pltpu.VMEM((*lq, n_fs, sub, wide), F32),
            pltpu.VMEM((*lq, n_fs, sub, wide), BF16),
            pltpu.VMEM((*lq, sub, wide), BF16),
            pltpu.VMEM((n_q, 2, sub, wide), BF16),
            pltpu.VMEM((n_q, 2, sub, wide), BF16),
            pltpu.VMEM((*lq, sub, wide), BF16),
            pltpu.VMEM((n_q, sub, wide), BF16),
            pltpu.VMEM((n_q, sub, wide), F32),
            pltpu.VMEM((n_q, sub, wide), BF16),
            pltpu.VMEM((n_q, rows_in, wide), BF16),
            dma, dma, dma, dma((2, 2)), dma(lq), dma,
            dma((2, n_fs)), dma((2, 2, 4)), dma((2,)), dma((2, 2, 4)),
            dma((2, n_fs)), dma((*lq, n_fs)), dma((2,)), dma(lq),
            dma((2,)), dma((2, n_fs, 2)), dma((2,)),
            dma((2,)), dma((2, n_fs, 2)), dma((2,)), dma((2,)), dma((2,)), dma((2,)),
            dma((2,)), dma((n_fs,)), dma((2,)),
            *[dma((2,)), dma(lq)] * 3, dma, dma((n_q,)), dma((2,)), dma(lq), dma, dma((n_q,)),
            dma, dma((n_q,)),
        ],
        compiler_params=pltpu.CompilerParams(
            collective_id=0, has_side_effects=True, vmem_limit_bytes=60 * 1024 * 1024),
    )(*args)


def fits(mesh, args):
    tokens, gate = args[0], args[3]
    n_tp = mesh.shape["tp"]
    return (mesh.shape["grp"] == 2 and mesh.shape["fs"] == 4 and n_tp == 4 and tokens.shape[0] % (32 * n_tp) == 0
            and gate.shape[0] % (128 * 4) == 0 and gate.shape[1] % 128 == 0)


def solution(mesh):
    n_fs, n_tp = mesh.shape["fs"], mesh.shape["tp"]

    def local(tokens, mix_heads, norm_first, gate_first, up_first, down_first, out_weight,
              norm_second, gate_second, up_second, down_second):
        args = (tokens, mix_heads, norm_first.reshape(1, -1), gate_first, up_first, down_first, out_weight,
                norm_second.reshape(1, -1), gate_second, up_second, down_second)
        if fits(mesh, args):
            return gathered_call(mesh, args)
        rows_in, width = tokens.shape
        total = rows_in * n_fs
        share = total // n_tp
        dc, hidden = gate_first.shape
        heads = mix_heads.shape[1]
        chunk = rows_in // 2
        n_chunks = total // 2 // chunk
        dma = pltpu.SemaphoreType.DMA
        vmem = pl.BlockSpec(memory_space=pltpu.VMEM)
        hbm = pl.BlockSpec(memory_space=pl.ANY)
        return pl.pallas_call(
            functools.partial(kernel, n_fs, n_tp, chunk),
            out_shape=jax.ShapeDtypeStruct((rows_in, width), BF16),
            in_specs=[vmem, vmem, vmem, hbm, hbm, hbm, hbm, vmem, hbm, hbm, hbm],
            out_specs=vmem,
            scratch_shapes=[
                pltpu.VMEM(gate_first.shape, BF16),
                pltpu.VMEM(up_first.shape, BF16),
                pltpu.VMEM(down_first.shape, BF16),
                pltpu.VMEM(out_weight.shape, BF16),
                pltpu.VMEM(gate_second.shape, BF16),
                pltpu.VMEM(up_second.shape, BF16),
                pltpu.VMEM(down_second.shape, BF16),
                pltpu.VMEM((total, dc), BF16),
                pltpu.VMEM((total, dc), BF16),
                pltpu.VMEM((total, heads), BF16),
                pltpu.VMEM((2, total, hidden), F32),
                pltpu.VMEM((2, total, hidden), BF16),
                pltpu.VMEM((2, total, hidden), BF16),
                pltpu.VMEM((2, total, hidden), BF16),
                pltpu.VMEM((total, hidden), BF16),
                pltpu.VMEM((total, hidden), BF16),
                pltpu.VMEM((total, dc), BF16),
                pltpu.VMEM((n_tp, share, dc), BF16),
                pltpu.VMEM((n_tp, share, dc), BF16),
                pltpu.VMEM((share, dc), F32),
                pltpu.VMEM((n_fs, 8, rows_in), F32),
                pltpu.VMEM((n_fs, 8, share), F32),
                pltpu.VMEM((share, dc), BF16),
                pltpu.VMEM((rows_in, width), BF16),
                dma((7,)), dma((n_fs,)), dma((n_fs,)), dma((n_fs,)), dma((n_fs,)), dma((n_fs,)), dma((n_fs,)),
                dma((n_fs, 2)), dma((n_fs,)),
                dma((2, 2, n_chunks)), dma((2, 2, n_chunks)), dma((2, 2, n_chunks)), dma((2, 2, n_chunks)),
                dma((2, n_tp)), dma((2, n_tp)),
                dma((n_fs,)), dma((n_fs,)), dma((n_tp,)), dma((n_tp,)), dma((n_tp,)), dma((n_tp,)),
                dma((n_tp,)), dma((n_fs,)), dma((n_fs,)), dma((n_fs,)),
            ],
            compiler_params=pltpu.CompilerParams(
                collective_id=0, has_side_effects=True, vmem_limit_bytes=60 * 1024 * 1024),
        )(*args)

    in_specs = (
        P(("grp", "fs"), None),
        P(("grp", "fs"), "tp"),
        P(),
        P("fs", "tp"),
        P("fs", "tp"),
        P("tp", "fs"),
        P("tp", "fs"),
        P(),
        P("fs", "tp"),
        P("fs", "tp"),
        P("tp", "fs"),
    )
    return jax.shard_map(local, mesh=mesh, in_specs=in_specs, out_specs=P(("grp", "fs"), None), check_vma=False)
```
